512 devices in a mesh: sp: 64 (over z, y), tp: 8 (over x, core).
Axes of the slice: x: 4, y: 4, z: 16, core: 2. Of those that a mesh axis runs over, the one named last changes fastest.
Arguments:
- tokens: bfloat16 [16384, 4096], P('sp'), may hold values from -5 to 5
- documents: int32 [16384], P('sp'), may hold values from 0 to 15, never falling along the last dimension, each value on 1 to 2048 neighbouring positions
- norm_gain: float32 [2, 4096], replicated, may hold values from 0.1 to 1.9
- in_weight: bfloat16 [2, 4096, 2048], P(None, 'sp', 'tp'), may hold values from -0.09375 to 0.09375
- conv_taps: float32 [2, 4, 2048], P(None, None, 'tp'), may hold values from -3 to 3
- conv_bias: float32 [2, 2048], P(None, 'tp'), may hold values from -0.75 to 0.75
- recur_gate: bfloat16 [2, 32, 64, 64], P(None, 'tp'), may hold values from -0.75 to 0.75
- input_gate: bfloat16 [2, 32, 64, 64], P(None, 'tp'), may hold values from -0.75 to 0.75
- recur_bias: float32 [2, 2048], P(None, 'tp'), may hold values from -4 to 4
- input_bias: float32 [2, 2048], P(None, 'tp'), may hold values from -4 to 4
- decay_param: float32 [2, 2048], P(None, 'tp'), may hold values from 4 to 7
- out_weight: bfloat16 [2, 2048, 4096], P(None, 'tp', 'sp'), may hold values from -0.375 to 0.375
Outputs:
- layered: bfloat16 [16384, 4096], P('sp')
The draws below stay inside these ranges and needn't reach their ends.
All inputs are finite; a program needn't handle non-finite values.
Results may differ from the reference program's by a relative error of at most 0.017.
Values may be sent and summed in bfloat16 or wider, within the bound.
A program may use at most 64 MiB of HBM per device.

```python
import math
import jax
import jax.numpy as jnp
import numpy as np
from jax import lax

D = 4096
RW = 2048
BD = 64
K = 4
LAYERS = 2
TOK_DEV = 256
TOKENS = 16384
NB = 32
N_SP = 64
N_TP = 8


def draw_tokens(key, part):
    scale_key, value_key, mean_key = jax.random.split(jax.random.fold_in(key, 11), 3)
    log_scale = jax.random.uniform(scale_key, (TOKENS // 128, 1), jnp.float32, -1.3863, -0.2877)
    block_scale = jnp.repeat(jnp.exp(log_scale), 128, axis=0)
    base = jax.random.normal(value_key, (TOKENS, D), jnp.float32)
    base = jnp.clip(base, -6.0, 6.0)
    return (base * block_scale).astype(jnp.bfloat16)


def draw_decay_param(key, part):
    flag_key, slow_key, fast_key = jax.random.split(jax.random.fold_in(key, 23), 3)
    picked = jax.random.randint(flag_key, (LAYERS, RW), 0, 2)
    slow_value = jax.random.uniform(slow_key, (LAYERS, RW), jnp.float32, 6.5, 7.0)
    fast_value = jax.random.uniform(fast_key, (LAYERS, RW), jnp.float32, 4.0, 5.0)
    return jnp.where(picked == 0, fast_value, slow_value)


def shard_levels(own_key, extent, pieces, smallest, high):
    gain = 1.0
    for dim, parts in pieces:
        draws = jax.random.uniform(jax.random.fold_in(jax.random.fold_in(own_key, 6), dim), (parts,), jnp.float32, smallest / len(pieces), high / len(pieces))
        gain = gain * jnp.repeat(jnp.exp(draws), extent[dim] // parts).reshape((-1,) + (1,) * (len(extent) - 1 - dim))
    return gain


def split_up(number_of, total, bound, lean):
    portions = [(1 << 20) // math.isqrt(standing ** lean) + 1 for standing in range(2, number_of + 1)]
    surplus, holding = total - bound - (number_of - 1), [1] * (number_of - 1)
    while surplus > 0:
        movable = [i for i in range(number_of - 1) if holding[i] < bound]
        mass, budget = sum([portions[i] for i in movable]), surplus
        for i in movable:
            addition = min(bound - holding[i], max(1, budget * portions[i] // mass), surplus)
            holding[i] = holding[i] + addition
            surplus = surplus - addition
    return np.array([bound] + holding)


def ragged(rng, number_of, total, most, slope):
    if number_of == 2:
        one = jax.random.randint(rng, (), max(1, total - most), min(most, total - 1) + 1)
        return jnp.stack([one, total - one])
    lengths = jnp.asarray(split_up(number_of, total, most, slope), jnp.int32)
    twos = (number_of - 1) // 2
    donor, sink = lengths[1:1 + 2 * twos:2], lengths[2:2 + 2 * twos:2]
    margin = jnp.minimum(donor - 1, most - sink)
    moved = jax.random.randint(jax.random.fold_in(rng, 1), (twos,), 0, 1 << 20) % (margin + 1)
    lengths = lengths.at[1:1 + 2 * twos:2].set(donor - moved).at[2:2 + 2 * twos:2].set(sink + moved)
    return lengths[jax.random.permutation(jax.random.fold_in(rng, 2), number_of)]


def bell_draw(rng, shape, scale, most, shards=(), kind=jnp.bfloat16):
    drawn = jax.random.normal(rng, shape, jnp.float32) * scale
    if len(shards) > 0:
        drawn = shard_levels(rng, shape, shards, -0.22, 0.18) * drawn
    return jnp.clip(drawn, min=-most, max=most).astype(kind)


def setup_inputs(seed: int = 0) -> dict:
    splits = jax.random.split(jax.random.key(seed), 13)
    tokens = draw_tokens(jax.random.fold_in(splits[12], 71), 0)
    documents = jnp.searchsorted(jnp.cumsum(ragged(splits[1], N_SP // 4, TOKENS, 8 * TOK_DEV, 0)), jnp.arange(TOKENS), side="right").astype(jnp.int32)
    norm_gain = jnp.clip(1.0 + 0.18 * jax.random.normal(splits[2], (LAYERS, D), jnp.float32), 0.1, 1.9)
    in_weight = bell_draw(splits[3], (LAYERS, D, RW), D ** -0.5, 0.09375, ((1, 64), (2, 8)))
    conv_taps = bell_draw(splits[4], (LAYERS, K, RW), K ** -0.5, 3.0, ((2, 8),), jnp.float32)
    conv_bias = bell_draw(splits[5], (LAYERS, RW), 0.05, 0.75, ((1, 8),), jnp.float32)
    recur_gate = bell_draw(splits[6], (LAYERS, NB, BD, BD), BD ** -0.5, 0.75, ((1, 8),))
    input_gate = bell_draw(splits[7], (LAYERS, NB, BD, BD), BD ** -0.5, 0.75, ((1, 8),))
    recur_bias = bell_draw(splits[8], (LAYERS, RW), 1.0, 4.0, ((1, 8),), jnp.float32)
    input_bias = bell_draw(splits[9], (LAYERS, RW), 1.0, 4.0, ((1, 8),), jnp.float32)
    decay_param = draw_decay_param(jax.random.fold_in(splits[12], 71), 0)
    out_weight = bell_draw(splits[11], (LAYERS, RW, D), (RW // 8) ** -0.5, 0.375, ((1, 8), (2, 64)))
    return {"tokens": tokens, "documents": documents, "norm_gain": norm_gain, "in_weight": in_weight, "conv_taps": conv_taps, "conv_bias": conv_bias, "recur_gate": recur_gate, "input_gate": input_gate, "recur_bias": recur_bias, "input_bias": input_bias, "decay_param": decay_param, "out_weight": out_weight}


RG_C = 8.0
EPS = 0.1

def norm_rows(values_in, gain_row):
    values = values_in.astype(jnp.float32)
    scaled = values * lax.rsqrt(lax.optimization_barrier(jnp.mean(values * values, axis=-1, keepdims=True)) + EPS)
    return (scaled * gain_row[None, :]).astype(jnp.bfloat16)

def combine(earlier, following):
    return (earlier[0] * following[0], following[0] * earlier[1] + following[1])

def reference(tokens, documents, norm_gain, in_weight, conv_taps, conv_bias, recur_gate, input_gate, recur_bias, input_bias, decay_param, out_weight):
    state_x = tokens
    prev_doc = jnp.concatenate([documents[:1], documents[:-1]])
    reset = documents != prev_doc
    group_width = RW // N_TP
    for depth_at in range(LAYERS):
        normed = norm_rows(state_x, norm_gain[depth_at])
        mixed_in = jnp.dot(normed, in_weight[depth_at], preferred_element_type=jnp.float32).astype(jnp.bfloat16)
        values_in = mixed_in.astype(jnp.float32)
        conv_sum = conv_bias[depth_at][None, :] + conv_taps[depth_at, 0][None, :] * values_in
        for lag_step in range(1, K):
            shifted = jnp.concatenate([jnp.zeros((lag_step, RW), jnp.float32), values_in[:-lag_step]], axis=0)
            shifted_doc = jnp.concatenate([jnp.full((lag_step,), -1, jnp.int32), documents[:-lag_step]], axis=0)
            same_doc = (shifted_doc == documents)[:, None]
            conv_sum = conv_sum + jnp.where(same_doc, conv_taps[depth_at, lag_step][None, :] * shifted, 0.0)
        conv_out = conv_sum.astype(jnp.bfloat16)
        grouped = conv_out.astype(jnp.float32).reshape(TOKENS, NB, BD)
        recur_rate = jax.nn.sigmoid(jnp.einsum('snb,nbc->snc', grouped, recur_gate[depth_at].astype(jnp.float32)).reshape(TOKENS, RW) + recur_bias[depth_at][None, :])
        input_rate = jax.nn.sigmoid(jnp.einsum('snb,nbc->snc', grouped, input_gate[depth_at].astype(jnp.float32)).reshape(TOKENS, RW) + input_bias[depth_at][None, :])
        log_decay = -RG_C * jax.nn.softplus(-decay_param[depth_at])[None, :] * recur_rate
        decay_now = jnp.where(reset[:, None], 0.0, jnp.exp(log_decay))
        drive_term = jnp.sqrt(jnp.maximum(-jnp.expm1(2.0 * log_decay), 0.0)) * (input_rate * conv_out.astype(jnp.float32))
        _, states = lax.associative_scan(combine, (decay_now, drive_term), axis=0)
        hidden = states.astype(jnp.bfloat16)
        summed = jnp.zeros((TOKENS, D), jnp.float32)
        for group in range(N_TP):
            low = group * group_width
            partial_term = jnp.dot(hidden[:, low:low + group_width], out_weight[depth_at, low:low + group_width], preferred_element_type=jnp.float32).astype(jnp.bfloat16)
            partial_term = lax.optimization_barrier(partial_term)
            summed = summed + partial_term.astype(jnp.float32)
        state_x = (state_x.astype(jnp.float32) + summed).astype(jnp.bfloat16)
    return state_x
```

```python
import functools

import jax
import jax.numpy as jnp
from jax import lax
from jax.experimental import pallas as pl
from jax.experimental.pallas import tpu as pltpu
from jax.sharding import PartitionSpec as P

RG_C = 8.0
EPS = 0.1
MESH = pl.DeviceIdType.MESH
F32 = jnp.float32
BF16 = jnp.bfloat16
NY = 4
NX = 4
BACK = 8
OFFSETS = (0, 4, 8, 12)


def nt_dot(a, b):
    return lax.dot_general(a, b, (((1,), (1,)), ((), ())), preferred_element_type=F32)


def kernel(
    n_sp, docs, tokens, gain, w_in, taps, conv_bias, rgate, igate, rbias, ibias, decay, w_out, out,
    wbuf, pdoc, dext, masks, gm, xg, x1, outb, acc, ss, ext, tail, a_s, b_s, h_s, p_s, hid,
    cown, cbuf, send_d, recv_d, send_x, recv_x, keep, own,
    z_recv, y_recv, z_send, y_send, d_sem, t_sem, c_recv, c_send, dr, ds, xr, xs, gr, gs, pr, ps, o_sem,
):
    rows, width = tokens.shape
    chans = taps.shape[2]
    blk = w_in.shape[1]
    half_l = chans // 2
    n_tp = 2 * NX
    cw = width // n_tp
    hr = rows // 2
    segs = 8
    steps = rows // segs
    n_z = n_sp // NY
    sp = lax.axis_index("sp")
    tp = lax.axis_index("tp")
    z, y = sp // NY, lax.rem(sp, NY)
    x, core = tp // 2, lax.rem(tp, 2)

    def at_y(d):
        return z * NY + lax.rem(y + d + NY, NY)

    def at_z(d):
        return lax.rem(z + d + n_z, n_z) * NY + y

    def at_sp(d):
        return lax.rem(sp + d + n_sp, n_sp)

    def at_x(d, c=0):
        return lax.rem(x + d + NX, NX) * 2 + (core if c == 0 else 1 - core)

    partner = x * 2 + (1 - core)
    xp, xm = at_x(1), at_x(-1)

    def rcopy(src, dst, ssem, rsem, to_sp, to_tp):
        pltpu.make_async_remote_copy(
            src_ref=src, dst_ref=dst, send_sem=ssem, recv_sem=rsem,
            device_id=(to_sp, to_tp), device_id_type=MESH,
        ).start()

    def wait(ref, sem):
        pltpu.make_async_copy(ref, ref, sem).wait()

    barrier = pltpu.get_barrier_semaphore()
    partners = [(at_y(1), tp), (at_y(-1), tp), (at_y(2), tp), (at_z(1), tp), (at_z(-1), tp)]
    partners += [(sp, xp), (sp, xm), (sp, partner)]
    partners += [(at_sp(d), tp) for k in range(1, BACK + 1) for d in (k, -k)]
    for to_sp, to_tp in partners:
        pl.semaphore_signal(barrier, inc=1, device_id=(to_sp, to_tp), device_id_type=MESH)

    eye = (
        lax.broadcasted_iota(jnp.int32, (blk, blk), 0) == lax.broadcasted_iota(jnp.int32, (blk, blk), 1)
    ).astype(BF16)
    mine = pl.ds(pl.multiple_of(sp * blk, blk), blk)
    for layer in range(2):
        w = w_in[layer]
        wt = nt_dot(eye, w_out[layer]).astype(BF16)
        for h in range(2):
            lanes = slice(h * half_l, (h + 1) * half_l)
            wbuf[2 * layer, h, mine, :] = w[:, lanes]
            wbuf[2 * layer + 1, h, mine, :] = wt[:, lanes]

    pl.semaphore_wait(barrier, len(partners))

    def block_rows(zz, yy):
        return pl.ds(pl.multiple_of((zz * NY + yy) * blk, blk), blk)

    def z_rows(zz):
        return pl.ds(pl.multiple_of(zz * NY * blk, NY * blk), NY * blk)

    def last_step(m, d):
        full = n_z // 2
        return full if (m + d) % 2 == 0 else full - 1

    def start_y(m):
        for d in (1, -1, 2):
            for h in range(2):
                piece = wbuf.at[m, h, mine, :]
                rcopy(piece, piece, y_send.at[m], y_recv.at[m, h], at_y(d), tp)

    def pass_first(m, d, zz):
        to = at_z(1 if d == 0 else -1)
        s_sem = z_send.at[m]
        return to, s_sem

    def fwd_first(m, d, s, zz):
        to, s_sem = pass_first(m, d, zz)
        r = block_rows(zz, y)
        piece = wbuf.at[m, :, r, :] if m == 0 else wbuf.at[m, 1, r, :]
        rcopy(piece, piece, s_sem, z_recv.at[m, d, s, 0], to, tp)

    def fwd_second(m, d, s, zz):
        to, s_sem = pass_first(m, d, zz)
        if m == 0:
            for dy in (1, -1, 2):
                piece = wbuf.at[m, 0, block_rows(zz, lax.rem(y + dy + NY, NY)), :]
                rcopy(piece, piece, s_sem, z_recv.at[m, d, s, 1], to, tp)
        else:
            piece = wbuf.at[m, 0, z_rows(zz), :]
            rcopy(piece, piece, s_sem, z_recv.at[m, d, s, 1], to, tp)

    first_rows = [2 * blk, blk, blk, blk]
    second_rows = [3 * blk, 4 * blk, 4 * blk, 4 * blk]

    def tick(m, s):
        if s == 0:
            for d in range(2):
                fwd_first(m, d, 1, z)
            start_y(m)
            wait(wbuf.at[m, 0, 0 : 3 * blk], y_recv.at[m, 0])
            for d in range(2):
                fwd_second(m, d, 1, z)
            return
        live = [d for d in range(2) if s <= last_step(m, d)]
        zs = {0: lax.rem(z - s + n_z, n_z), 1: lax.rem(z + s, n_z)}
        for d in live:
            wait(wbuf.at[m, 0, 0 : first_rows[m]], z_recv.at[m, d, s, 0])
            if s < last_step(m, d):
                fwd_first(m, d, s + 1, zs[d])
            piece = wbuf.at[m, 1, block_rows(zs[d], y), :]
            for dy in (1, -1, 2):
                rcopy(piece, piece, y_send.at[m], y_recv.at[m, 1], at_y(dy), tp)
        for d in live:
            wait(wbuf.at[m, 0, 0 : second_rows[m]], z_recv.at[m, d, s, 1])
            if s < last_step(m, d):
                fwd_second(m, d, s + 1, zs[d])

    done = [0]

    def run_ticks(upto):
        while done[0] < upto:
            t = done[0]
            for m in range(4):
                if 0 <= t - OFFSETS[m] <= n_z // 2:
                    tick(m, t - OFFSETS[m])
            done[0] += 1

    def have(m):
        run_ticks(OFFSETS[m] + n_z // 2 + 1)
        wait(wbuf.at[m, 0, 0 : (n_z * 3) * blk], y_recv.at[m, 1])

    def wrows(m, q):
        r = pl.ds(pl.multiple_of(q * cw, cw), cw)
        return jnp.concatenate([wbuf[m, 0, r, :], wbuf[m, 1, r, :]], axis=1)

    rcopy(docs, pdoc, d_sem.at[0], d_sem.at[1], at_sp(1), tp)
    run_ticks(1)

    ss[...] = jnp.zeros_like(ss)
    acc[...] = jnp.zeros_like(acc)

    def scaled(layer, values, q):
        v = values.astype(F32)
        sq = v * v
        part = sq[:, 0:128]
        for i in range(1, cw // 128):
            part = part + sq[:, i * 128 : (i + 1) * 128]
        ss[...] += part
        g = gain[layer : layer + 1, pl.ds(pl.multiple_of(q * cw, cw), cw)]
        return (v * g).astype(BF16)

    def prepare(q, _):
        xg[q] = scaled(0, tokens[:, pl.ds(pl.multiple_of(q * cw, cw), cw)], q)
        return 0

    lax.fori_loop(0, n_tp, prepare, 0)
    run_ticks(2)

    bd = rgate.shape[2]
    spread = (
        lax.rem(lax.broadcasted_iota(jnp.int32, (bd, chans), 1), bd)
        == lax.broadcasted_iota(jnp.int32, (bd, chans), 0)
    ).astype(BF16)
    on_block = (
        lax.broadcasted_iota(jnp.int32, (chans, chans), 0) // bd
        == lax.broadcasted_iota(jnp.int32, (chans, chans), 1) // bd
    )
    for layer in range(2):
        for i, g in enumerate((rgate, igate)):
            tiled = jnp.dot(g[layer], spread, preferred_element_type=F32)
            gm[layer, :, i * chans : (i + 1) * chans] = jnp.where(on_block, tiled, 0.0).astype(BF16)
    run_ticks(3)

    wait(pdoc, d_sem.at[1])
    eye_r = (
        lax.broadcasted_iota(jnp.int32, (rows, rows), 0) == lax.broadcasted_iota(jnp.int32, (rows, rows), 1)
    ).astype(BF16)
    own_docs = jnp.broadcast_to(docs[...], (128, rows)).astype(F32).astype(BF16)
    prev_docs = jnp.broadcast_to(pdoc[...], (128, rows)).astype(F32).astype(BF16)
    dext[8:, :] = nt_dot(eye_r, own_docs)
    before = nt_dot(eye_r[rows - 8 :, :], prev_docs)
    first_dev = jnp.broadcast_to((sp == 0).astype(F32), (8, 128))
    dext[0:8, :] = before * (1.0 - first_dev) - first_dev
    for k in range(1, 4):
        masks[k - 1] = (dext[8 - k : 8 - k + rows, :] == dext[8:, :]).astype(F32)

    def put(ref, value):
        for i in range(chans // 128):
            ref[i] = value[:, i * 128 : (i + 1) * 128]

    def across(ref, j):
        return jnp.concatenate(
            [ref[i, pl.ds(j, segs, stride=steps), :] for i in range(chans // 128)], axis=1
        )

    def layer_front(layer):
        r = lax.rsqrt(jnp.sum(ss[...], axis=1, keepdims=True) * (1.0 / width) + EPS)
        mixed = (acc[...] * r).astype(BF16).astype(F32)
        ext[8:, :] = mixed
        rcopy(ext.at[rows : rows + 8, :], tail.at[layer], t_sem.at[layer, 0], t_sem.at[layer, 1], at_sp(1), tp)
        wait(tail.at[layer], t_sem.at[layer, 1])
        wait(tail.at[layer], t_sem.at[layer, 0])
        ext[0:8, :] = tail[layer]

        def wide(mask):
            return jnp.concatenate([mask] * (chans // 128), axis=1)

        conv = conv_bias[layer : layer + 1, :] + taps[layer, 0:1, :] * mixed
        for k in range(1, 4):
            conv = conv + wide(masks[k - 1]) * (taps[layer, k : k + 1, :] * ext[8 - k : 8 - k + rows, :])
        conv_b = conv.astype(BF16)
        conv_f = conv_b.astype(F32)
        logits = jnp.dot(conv_b, gm[layer], preferred_element_type=F32)
        rr = jax.nn.sigmoid(logits[:, :chans] + rbias[layer : layer + 1, :])
        ir = jax.nn.sigmoid(logits[:, chans:] + ibias[layer : layer + 1, :])
        dp = decay[layer : layer + 1, :]
        soft = jnp.maximum(-dp, 0.0) + jnp.log1p(jnp.exp(-jnp.abs(dp)))
        log_decay = (-RG_C * soft) * rr
        put(a_s, jnp.exp(log_decay) * wide(masks[0]))
        u = -2.0 * log_decay
        series = 1.0 - u * (1.0 / 8.0)
        for n in (7, 6, 5, 4, 3, 2):
            series = 1.0 - (u * (1.0 / n)) * series
        gone = jnp.where(u < 0.35, u * series, 1.0 - jnp.exp(-u))
        put(b_s, jnp.sqrt(jnp.maximum(gone, 0.0)) * (ir * conv_f))
        h = jnp.zeros((segs, chans), F32)
        p = jnp.ones((segs, chans), F32)
        for j in range(steps):
            a_j = across(a_s, j)
            h = a_j * h + across(b_s, j)
            p = p * a_j
            h_s[j] = h
            p_s[j] = p
        al = jnp.ones((1, chans), F32)
        be = jnp.zeros((1, chans), F32)
        als, bes = [al], [be]
        for s in range(segs):
            ps_, hs_ = p[s : s + 1, :], h[s : s + 1, :]
            be = ps_ * be + hs_
            al = ps_ * al
            als.append(al)
            bes.append(be)
        cown[layer, 0:1, :] = al
        cown[layer, 1:2, :] = be
        for k in range(1, BACK + 1):
            rcopy(cown.at[layer], cbuf.at[layer, k - 1], c_send.at[layer], c_recv.at[layer, k - 1], at_sp(k), tp)
        c_in = jnp.zeros((1, chans), F32)
        for k in range(BACK, 0, -1):
            wait(cbuf.at[layer, k - 1], c_recv.at[layer, k - 1])
            c_in = cbuf[layer, k - 1, 0:1, :] * c_in + cbuf[layer, k - 1, 1:2, :]
        carry = jnp.concatenate([als[s] * c_in + bes[s] for s in range(segs)], axis=0)
        for j in range(steps):
            value = h_s[j] + p_s[j] * carry
            for i in range(chans // 128):
                hid[i, pl.ds(j, segs, stride=steps), :] = value[:, i * 128 : (i + 1) * 128]
        return jnp.concatenate([hid[i].astype(BF16) for i in range(chans // 128)], axis=1)

    def layer_back(layer, hidden, state_chunk, big, arrived):
        m = 2 * layer + 1
        order = (2, 1, -1, 0)
        for j, d in enumerate(order):
            part = nt_dot(hidden, wrows(m, at_x(d, 1)))
            send_d[layer, j] = part.astype(BF16)
            rcopy(send_d.at[layer, j], recv_d.at[layer, j], ds.at[layer, j], dr.at[layer, j], sp, partner)

        def send_half(i, value, to):
            send_x[layer, i] = value.astype(BF16)
            rcopy(send_x.at[layer, i], recv_x.at[layer, i], xs.at[layer, i], xr.at[layer, i], sp, to)

        for j, d in enumerate(order):
            part = nt_dot(hidden, wrows(m, at_x(d)))
            wait(recv_d.at[layer, j], dr.at[layer, j])
            both = part + recv_d[layer, j].astype(F32)
            if j == 0:
                send_half(0, both[:hr], xp)
                send_half(1, both[hr:], xm)
            elif j == 1:
                send_half(2, both[hr:], xp)
                keep[:hr, :] = both[:hr]
            elif j == 2:
                send_half(3, both[:hr], xm)
                keep[hr:, :] = both[hr:]
            else:
                own[...] = both + state_chunk().astype(F32)
        for i, to in ((0, xp), (1, xm)):
            half = slice(0, hr) if i == 0 else slice(hr, rows)
            wait(recv_x.at[layer, i], xr.at[layer, i])
            send_half(4 + i, keep[half, :] + recv_x[layer, i].astype(F32), to)
        for i in (2, 3):
            wait(recv_x.at[layer, i], xr.at[layer, i])
        top = own[:hr, :] + recv_x[layer, 3].astype(F32)
        bottom = own[hr:, :] + recv_x[layer, 2].astype(F32)
        wait(recv_x.at[layer, 4], xr.at[layer, 4])
        big[tp, 0:hr, :] = (top + recv_x[layer, 4].astype(F32)).astype(BF16)
        wait(recv_x.at[layer, 5], xr.at[layer, 5])
        big[tp, hr:rows, :] = (bottom + recv_x[layer, 5].astype(F32)).astype(BF16)

        def to_partner(i, q):
            rcopy(big.at[q], big.at[q], ps.at[layer, i], pr.at[layer, i], sp, partner)

        for i, to in ((0, xp), (1, xm)):
            rcopy(big.at[tp], big.at[tp], gs.at[layer, i], gr.at[layer, i], sp, to)
        to_partner(0, tp)
        arrived(tp)
        for i, (q, to) in enumerate(((xm, xp), (xp, xm))):
            half = slice(0, hr) if i == 0 else slice(hr, rows)
            wait(big.at[q], gr.at[layer, i])
            rcopy(big.at[q, half, :], big.at[q, half, :], gs.at[layer, 2 + i], gr.at[layer, 2 + i], sp, to)
            to_partner(1 + i, q)
        wait(big.at[partner], pr.at[layer, 0])
        arrived(partner)
        for i, d in enumerate((-1, 1)):
            arrived(at_x(d))
            wait(big.at[at_x(d, 1)], pr.at[layer, 1 + i])
            arrived(at_x(d, 1))
        far = at_x(2)
        wait(big.at[far, 0:hr, :], gr.at[layer, 2])
        wait(big.at[far, hr:rows, :], gr.at[layer, 3])
        to_partner(3, far)
        arrived(far)
        wait(big.at[at_x(2, 1)], pr.at[layer, 3])
        arrived(at_x(2, 1))

    have(0)

    def project(q, _):
        acc[...] += jnp.dot(xg[q], wrows(0, q), preferred_element_type=F32)
        return 0

    lax.fori_loop(0, n_tp, project, 0)
    hidden = layer_front(0)
    have(1)
    have(2)
    have(3)
    ss[...] = jnp.zeros_like(ss)
    acc[...] = jnp.zeros_like(acc)

    def absorb(q):
        acc[...] += jnp.dot(scaled(1, x1[q], q), wrows(2, q), preferred_element_type=F32)

    def token_chunk():
        return tokens[:, pl.ds(pl.multiple_of(tp * cw, cw), cw)]

    layer_back(0, hidden, token_chunk, x1, absorb)

    hidden = layer_front(1)

    def write_out(q):
        pltpu.make_async_copy(
            outb.at[q], out.at[:, pl.ds(pl.multiple_of(q * cw, cw), cw)], o_sem.at[q]
        ).start()

    layer_back(1, hidden, lambda: x1[tp], outb, write_out)

    for q in range(n_tp):
        pltpu.make_async_copy(outb.at[q], out.at[:, q * cw : (q + 1) * cw], o_sem.at[q]).wait()
    for m in range(4):
        n_hops = n_z - 1
        wait(wbuf.at[m, :, 0 : n_hops * 5 * blk // 2], z_send.at[m])
        wait(wbuf.at[m, :, 0 : (3 + 3 * n_z) * blk // 2], y_send.at[m])
    wait(docs, d_sem.at[0])
    for layer in range(2):
        wait(cbuf.at[layer], c_send.at[layer])
        for j in range(4):
            wait(send_d.at[layer, j], ds.at[layer, j])
            wait(outb.at[j], ps.at[layer, j])
            wait(outb.at[j] if j < 2 else outb.at[j, 0:hr, :], gs.at[layer, j])
        for j in range(6):
            wait(send_x.at[layer, j], xs.at[layer, j])


def per_device(
    n_sp, tokens, documents, norm_gain, in_weight, conv_taps, conv_bias, recur_gate, input_gate,
    recur_bias, input_bias, decay_param, out_weight,
):
    rows, width = tokens.shape
    layers, blk, chans = in_weight.shape
    n_tp = 2 * NX
    cw = width // n_tp
    hr = rows // 2
    flat = (layers, chans, recur_gate.shape[3])
    vmem = pl.BlockSpec(memory_space=pltpu.VMEM)
    big = pltpu.VMEM((n_tp, rows, cw), BF16)
    square = pltpu.VMEM((rows, chans), F32)
    lanes = pltpu.VMEM((chans // 128, rows, 128), F32)
    strided = pltpu.VMEM((rows // 8, 8, chans), F32)
    dma = pltpu.SemaphoreType.DMA
    scratch = [
        pltpu.VMEM((4, 2, width, chans // 2), BF16),
        pltpu.VMEM((1, rows), jnp.int32),
        pltpu.VMEM((rows + 8, 128), F32),
        pltpu.VMEM((3, rows, 128), F32),
        pltpu.VMEM((layers, chans, 2 * chans), BF16),
        big,
        big,
        big,
        square,
        pltpu.VMEM((rows, 128), F32),
        pltpu.VMEM((rows + 8, chans), F32),
        pltpu.VMEM((layers, 8, chans), F32),
        lanes,
        lanes,
        strided,
        strided,
        lanes,
        pltpu.VMEM((layers, 2, chans), F32),
        pltpu.VMEM((layers, BACK, 2, chans), F32),
        pltpu.VMEM((layers, 4, rows, cw), BF16),
        pltpu.VMEM((layers, 4, rows, cw), BF16),
        pltpu.VMEM((layers, 6, hr, cw), BF16),
        pltpu.VMEM((layers, 6, hr, cw), BF16),
        pltpu.VMEM((rows, cw), F32),
        pltpu.VMEM((rows, cw), F32),
        dma((4, 2, n_sp // NY // 2 + 1, 2)),
        dma((4, 2)),
        dma((4,)),
        dma((4,)),
        dma((2,)),
        dma((layers, 2)),
        dma((layers, BACK)),
        dma((layers,)),
        dma((layers, 4)),
        dma((layers, 4)),
        dma((layers, 6)),
        dma((layers, 6)),
        dma((layers, 4)),
        dma((layers, 4)),
        dma((layers, 4)),
        dma((layers, 4)),
        dma((n_tp,)),
    ]
    return pl.pallas_call(
        functools.partial(kernel, n_sp),
        out_shape=jax.ShapeDtypeStruct((rows, width), BF16),
        in_specs=[vmem] * 12,
        out_specs=pl.BlockSpec(memory_space=pl.ANY),
        scratch_shapes=scratch,
        compiler_params=pltpu.CompilerParams(
            collective_id=0, has_side_effects=True, vmem_limit_bytes=56 * 1024 * 1024
        ),
    )(
        documents.reshape(1, rows), tokens, norm_gain, in_weight, conv_taps, conv_bias,
        recur_gate.reshape(flat), input_gate.reshape(flat), recur_bias, input_bias, decay_param, out_weight,
    )


def solution(mesh):
    return jax.shard_map(
        functools.partial(per_device, mesh.shape["sp"]),
        mesh=mesh,
        in_specs=(
            P("sp", None),
            P("sp"),
            P(),
            P(None, "sp", "tp"),
            P(None, None, "tp"),
            P(None, "tp"),
            P(None, "tp", None, None),
            P(None, "tp", None, None),
            P(None, "tp"),
            P(None, "tp"),
            P(None, "tp"),
            P(None, "tp", "sp"),
        ),
        out_specs=P("sp", None),
        check_vma=False,
    )
```

```python
import functools

import jax
import jax.numpy as jnp
from jax import lax
from jax.experimental import pallas as pl
from jax.experimental.pallas import tpu as pltpu
from jax.sharding import PartitionSpec as P

RG_C = 8.0
EPS = 0.1
MESH = pl.DeviceIdType.MESH
F32 = jnp.float32
BF16 = jnp.bfloat16
NY = 4
NX = 4
BACK = 8
SCHEDULE = {f"t{t}": [(0, t)] for t in range(9)}
for t in range(3, 9):
    SCHEDULE[f"t{t}"].append((1, t - 3))
for t in range(6, 9):
    SCHEDULE[f"t{t}"].append((2, t - 6))
SCHEDULE |= {
    "f0a": [(1, 6)],
    "f0b": [(1, 7), (2, 3)],
    "f0c": [(1, 8), (2, 4)],
    "b0a": [(2, 5)],
    "b0b": [(2, 6), (3, 0)],
    "b0c": [(2, 7)],
    "b0d": [(2, 8), (3, 1)],
    "g0a": [(3, 2)],
    "g0b": [(3, 3)],
    "g0c": [(3, 4)],
    "f1a": [(3, 5)],
    "f1b": [(3, 6)],
    "f1c": [(3, 7)],
    "b1": [(3, 8)],
}


def nt_dot(a, b):
    return lax.dot_general(a, b, (((1,), (1,)), ((), ())), preferred_element_type=F32)


def kernel(
    n_sp, docs, tokens, gain, w_in, taps, conv_bias, rgate, igate, rbias, ibias, decay, w_out, out,
    wbuf, pdoc, dext, masks, gm, xg, x1, outb, acc, ss, ext, tail, a_s, b_s, h_s, p_s, hid,
    cown, cbuf, send_d, recv_d, send_x, recv_x, keep, own, part,
    z_recv, y_recv, z_send, y_send, d_sem, t_sem, c_recv, c_send, dr, ds, xr, xs, gr, gs, pr, ps, o_sem,
):
    rows, width = tokens.shape
    chans = taps.shape[2]
    blk = w_in.shape[1]
    half_l = chans // 2
    n_tp = 2 * NX
    cw = width // n_tp
    hr = rows // 2
    segs = 8
    steps = rows // segs
    n_z = n_sp // NY
    sp = lax.axis_index("sp")
    tp = lax.axis_index("tp")
    z, y = sp // NY, lax.rem(sp, NY)
    x, core = tp // 2, lax.rem(tp, 2)

    def at_y(d):
        return z * NY + lax.rem(y + d + NY, NY)

    def at_z(d):
        return lax.rem(z + d + n_z, n_z) * NY + y

    def at_sp(d):
        return lax.rem(sp + d + n_sp, n_sp)

    def at_x(d, c=0):
        return lax.rem(x + d + NX, NX) * 2 + (core if c == 0 else 1 - core)

    partner = x * 2 + (1 - core)
    xp, xm = at_x(1), at_x(-1)

    def rcopy(src, dst, ssem, rsem, to_sp, to_tp):
        pltpu.make_async_remote_copy(
            src_ref=src, dst_ref=dst, send_sem=ssem, recv_sem=rsem,
            device_id=(to_sp, to_tp), device_id_type=MESH,
        ).start()

    def wait(ref, sem):
        pltpu.make_async_copy(ref, ref, sem).wait()

    barrier = pltpu.get_barrier_semaphore()
    partners = [(at_y(1), tp), (at_y(-1), tp), (at_y(2), tp), (at_z(1), tp), (at_z(-1), tp)]
    partners += [(sp, xp), (sp, xm), (sp, partner)]
    partners += [(at_sp(d), tp) for k in range(1, BACK + 1) for d in (k, -k)]
    for to_sp, to_tp in partners:
        pl.semaphore_signal(barrier, inc=1, device_id=(to_sp, to_tp), device_id_type=MESH)

    mine = pl.ds(pl.multiple_of(sp * blk, blk), blk)
    for layer in range(2):
        w = w_in[layer]
        wt = w_out[layer]
        for h in range(2):
            lanes = slice(h * half_l, (h + 1) * half_l)
            wbuf[2 * layer, h, mine, :] = w[:, lanes]
            wbuf[2 * layer + 1, h, mine, :] = wt[:, lanes]

    pl.semaphore_wait(barrier, len(partners))

    def block_rows(zz, yy):
        return pl.ds(pl.multiple_of((zz * NY + yy) * blk, blk), blk)

    def z_rows(zz):
        return pl.ds(pl.multiple_of(zz * NY * blk, NY * blk), NY * blk)

    def last_step(m, d):
        full = n_z // 2
        return full if (m + d) % 2 == 0 else full - 1

    def start_y(m):
        for d in (1, -1, 2):
            for h in range(2):
                piece = wbuf.at[m, h, mine, :]
                rcopy(piece, piece, y_send.at[m], y_recv.at[m, h], at_y(d), tp)

    def pass_first(m, d, zz):
        to = at_z(1 if d == 0 else -1)
        s_sem = z_send.at[m]
        return to, s_sem

    def fwd_first(m, d, s, zz):
        to, s_sem = pass_first(m, d, zz)
        r = block_rows(zz, y)
        piece = wbuf.at[m, :, r, :] if m == 0 else wbuf.at[m, 1, r, :]
        rcopy(piece, piece, s_sem, z_recv.at[m, d, s, 0], to, tp)

    def fwd_second(m, d, s, zz):
        to, s_sem = pass_first(m, d, zz)
        if m == 0:
            for dy in (1, -1, 2):
                piece = wbuf.at[m, 0, block_rows(zz, lax.rem(y + dy + NY, NY)), :]
                rcopy(piece, piece, s_sem, z_recv.at[m, d, s, 1], to, tp)
        else:
            piece = wbuf.at[m, 0, z_rows(zz), :]
            rcopy(piece, piece, s_sem, z_recv.at[m, d, s, 1], to, tp)

    first_rows = [2 * blk, blk, blk, blk]
    second_rows = [3 * blk, 4 * blk, 4 * blk, 4 * blk]

    def tick(m, s):
        if s == 0:
            for d in range(2):
                fwd_first(m, d, 1, z)
            start_y(m)
            wait(wbuf.at[m, 0, 0 : 3 * blk], y_recv.at[m, 0])
            for d in range(2):
                fwd_second(m, d, 1, z)
            return
        live = [d for d in range(2) if s <= last_step(m, d)]
        zs = {0: lax.rem(z - s + n_z, n_z), 1: lax.rem(z + s, n_z)}
        for d in live:
            wait(wbuf.at[m, 0, 0 : first_rows[m]], z_recv.at[m, d, s, 0])
            if s < last_step(m, d):
                fwd_first(m, d, s + 1, zs[d])
            piece = wbuf.at[m, 1, block_rows(zs[d], y), :]
            for dy in (1, -1, 2):
                rcopy(piece, piece, y_send.at[m], y_recv.at[m, 1], at_y(dy), tp)
        for d in live:
            wait(wbuf.at[m, 0, 0 : second_rows[m]], z_recv.at[m, d, s, 1])
            if s < last_step(m, d):
                fwd_second(m, d, s + 1, zs[d])

    def run(point):
        for m, step in SCHEDULE.get(point, ()):
            tick(m, step)

    def have(m):
        wait(wbuf.at[m, 0, 0 : (n_z * 3) * blk], y_recv.at[m, 1])

    def wrows(m, q):
        r = pl.ds(pl.multiple_of(q * cw, cw), cw)
        return jnp.concatenate([wbuf[m, 0, r, :], wbuf[m, 1, r, :]], axis=1)

    rcopy(docs, pdoc, d_sem.at[0], d_sem.at[1], at_sp(1), tp)
    run("t0")

    ss[...] = jnp.zeros_like(ss)
    acc[...] = jnp.zeros_like(acc)

    def scaled(layer, values, q):
        v = values.astype(F32)
        sq = v * v
        part = sq[:, 0:128]
        for i in range(1, cw // 128):
            part = part + sq[:, i * 128 : (i + 1) * 128]
        ss[...] += part
        g = gain[layer : layer + 1, pl.ds(pl.multiple_of(q * cw, cw), cw)]
        return (v * g).astype(BF16)

    def prepare(q, _):
        xg[q] = scaled(0, tokens[:, pl.ds(pl.multiple_of(q * cw, cw), cw)], q)
        return 0

    lax.fori_loop(0, n_tp, prepare, 0)
    run("t1")

    bd = rgate.shape[2]
    spread = (
        lax.rem(lax.broadcasted_iota(jnp.int32, (bd, chans), 1), bd)
        == lax.broadcasted_iota(jnp.int32, (bd, chans), 0)
    ).astype(BF16)
    on_block = (
        lax.broadcasted_iota(jnp.int32, (chans, chans), 0) // bd
        == lax.broadcasted_iota(jnp.int32, (chans, chans), 1) // bd
    )
    for layer in range(2):
        for i, g in enumerate((rgate, igate)):
            tiled = jnp.dot(g[layer], spread, preferred_element_type=F32)
            gm[layer, :, i * chans : (i + 1) * chans] = jnp.where(on_block, tiled, 0.0).astype(BF16)
    run("t2")

    wait(pdoc, d_sem.at[1])
    eye_r = (
        lax.broadcasted_iota(jnp.int32, (rows, rows), 0) == lax.broadcasted_iota(jnp.int32, (rows, rows), 1)
    ).astype(BF16)
    own_docs = jnp.broadcast_to(docs[...], (128, rows)).astype(F32).astype(BF16)
    prev_docs = jnp.broadcast_to(pdoc[...], (128, rows)).astype(F32).astype(BF16)
    dext[8:, :] = nt_dot(eye_r, own_docs)
    before = nt_dot(eye_r[rows - 8 :, :], prev_docs)
    first_dev = jnp.broadcast_to((sp == 0).astype(F32), (8, 128))
    dext[0:8, :] = before * (1.0 - first_dev) - first_dev
    for k in range(1, 4):
        masks[k - 1] = (dext[8 - k : 8 - k + rows, :] == dext[8:, :]).astype(F32)

    def put(ref, value):
        for i in range(chans // 128):
            ref[i] = value[:, i * 128 : (i + 1) * 128]

    def across(ref, j):
        return jnp.concatenate(
            [ref[i, pl.ds(j, segs, stride=steps), :] for i in range(chans // 128)], axis=1
        )

    def layer_front(layer):
        r = lax.rsqrt(jnp.sum(ss[...], axis=1, keepdims=True) * (1.0 / width) + EPS)
        mixed = (acc[...] * r).astype(BF16).astype(F32)
        ext[8:, :] = mixed
        rcopy(ext.at[rows : rows + 8, :], tail.at[layer], t_sem.at[layer, 0], t_sem.at[layer, 1], at_sp(1), tp)
        run(f"f{layer}a")
        wait(tail.at[layer], t_sem.at[layer, 1])
        wait(tail.at[layer], t_sem.at[layer, 0])
        ext[0:8, :] = tail[layer]

        def wide(mask):
            return jnp.concatenate([mask] * (chans // 128), axis=1)

        conv = conv_bias[layer : layer + 1, :] + taps[layer, 0:1, :] * mixed
        for k in range(1, 4):
            conv = conv + wide(masks[k - 1]) * (taps[layer, k : k + 1, :] * ext[8 - k : 8 - k + rows, :])
        conv_b = conv.astype(BF16)
        conv_f = conv_b.astype(F32)
        logits = jnp.dot(conv_b, gm[layer], preferred_element_type=F32)
        rr = jax.nn.sigmoid(logits[:, :chans] + rbias[layer : layer + 1, :])
        ir = jax.nn.sigmoid(logits[:, chans:] + ibias[layer : layer + 1, :])
        dp = decay[layer : layer + 1, :]
        soft = jnp.maximum(-dp, 0.0) + jnp.log1p(jnp.exp(-jnp.abs(dp)))
        log_decay = (-RG_C * soft) * rr
        put(a_s, jnp.exp(log_decay) * wide(masks[0]))
        u = -2.0 * log_decay
        series = 1.0 - u * (1.0 / 8.0)
        for n in (7, 6, 5, 4, 3, 2):
            series = 1.0 - (u * (1.0 / n)) * series
        gone = jnp.where(u < 0.35, u * series, 1.0 - jnp.exp(-u))
        put(b_s, jnp.sqrt(jnp.maximum(gone, 0.0)) * (ir * conv_f))
        run(f"f{layer}b")
        h = jnp.zeros((segs, chans), F32)
        p = jnp.ones((segs, chans), F32)
        for j in range(steps):
            a_j = across(a_s, j)
            h = a_j * h + across(b_s, j)
            p = p * a_j
            h_s[j] = h
            p_s[j] = p
        al = jnp.ones((1, chans), F32)
        be = jnp.zeros((1, chans), F32)
        als, bes = [al], [be]
        for s in range(segs):
            ps_, hs_ = p[s : s + 1, :], h[s : s + 1, :]
            be = ps_ * be + hs_
            al = ps_ * al
            als.append(al)
            bes.append(be)
        cown[layer, 0:1, :] = al
        cown[layer, 1:2, :] = be
        for k in range(1, BACK + 1):
            rcopy(cown.at[layer], cbuf.at[layer, k - 1], c_send.at[layer], c_recv.at[layer, k - 1], at_sp(k), tp)
        run(f"f{layer}c")
        c_in = jnp.zeros((1, chans), F32)
        for k in range(BACK, 0, -1):
            wait(cbuf.at[layer, k - 1], c_recv.at[layer, k - 1])
            c_in = cbuf[layer, k - 1, 0:1, :] * c_in + cbuf[layer, k - 1, 1:2, :]
        carry = jnp.concatenate([als[s] * c_in + bes[s] for s in range(segs)], axis=0)
        for j in range(steps):
            value = h_s[j] + p_s[j] * carry
            for i in range(chans // 128):
                hid[i, pl.ds(j, segs, stride=steps), :] = value[:, i * 128 : (i + 1) * 128]
        return jnp.concatenate([hid[i].astype(BF16) for i in range(chans // 128)], axis=1)

    def layer_back(layer, hidden, state_chunk, big, arrived):
        m = 2 * layer + 1
        run(f"b{layer}")
        have(m)
        order = (2, 1, -1, 0)

        def for_partner(j):
            send_d[layer, j] = nt_dot(hidden, wrows(m, at_x(order[j], 1))).astype(BF16)
            rcopy(send_d.at[layer, j], recv_d.at[layer, j], ds.at[layer, j], dr.at[layer, j], sp, partner)

        def for_self(j):
            part[j] = nt_dot(hidden, wrows(m, at_x(order[j])))

        def of_chip(j):
            wait(recv_d.at[layer, j], dr.at[layer, j])
            return part[j] + recv_d[layer, j].astype(F32)

        def send_half(i, value, to):
            send_x[layer, i] = value.astype(BF16)
            rcopy(send_x.at[layer, i], recv_x.at[layer, i], xs.at[layer, i], xr.at[layer, i], sp, to)

        for_partner(0)
        for_self(0)
        for_partner(1)
        both = of_chip(0)
        send_half(0, both[:hr], xp)
        send_half(1, both[hr:], xm)
        for_self(1)
        for_partner(2)
        run(f"b{layer}a")
        both = of_chip(1)
        send_half(2, both[hr:], xp)
        keep[:hr, :] = both[:hr]
        for_self(2)
        for_partner(3)
        both = of_chip(2)
        send_half(3, both[:hr], xm)
        keep[hr:, :] = both[hr:]
        for_self(3)
        run(f"b{layer}b")
        own[...] = of_chip(3) + state_chunk().astype(F32)
        run(f"b{layer}c")
        for i, to in ((0, xp), (1, xm)):
            half = slice(0, hr) if i == 0 else slice(hr, rows)
            wait(recv_x.at[layer, i], xr.at[layer, i])
            send_half(4 + i, keep[half, :] + recv_x[layer, i].astype(F32), to)
        run(f"b{layer}d")
        for i in (2, 3):
            wait(recv_x.at[layer, i], xr.at[layer, i])
        top = own[:hr, :] + recv_x[layer, 3].astype(F32)
        bottom = own[hr:, :] + recv_x[layer, 2].astype(F32)

        def half_of(q, h):
            return big.at[q, h * hr : (h + 1) * hr, :]

        def to_x(i, q, h, to):
            rcopy(half_of(q, h), half_of(q, h), gs.at[layer, i], gr.at[layer, i], sp, to)

        def to_partner(i, q):
            rcopy(big.at[q], big.at[q], ps.at[layer, i], pr.at[layer, i], sp, partner)

        wait(recv_x.at[layer, 4], xr.at[layer, 4])
        big[tp, 0:hr, :] = (top + recv_x[layer, 4].astype(F32)).astype(BF16)
        to_x(0, tp, 0, xp)
        wait(recv_x.at[layer, 5], xr.at[layer, 5])
        big[tp, hr:rows, :] = (bottom + recv_x[layer, 5].astype(F32)).astype(BF16)
        to_x(1, tp, 1, xm)
        to_x(2, tp, 1, xp)
        to_x(3, tp, 0, xm)
        to_partner(0, tp)
        if layer == 0:
            have(2)
        arrived(tp)
        run(f"g{layer}a")
        wait(half_of(xm, 0), gr.at[layer, 0])
        to_x(4, xm, 0, xp)
        wait(half_of(xp, 1), gr.at[layer, 1])
        to_x(5, xp, 1, xm)
        wait(half_of(xm, 1), gr.at[layer, 2])
        to_partner(1, xm)
        wait(half_of(xp, 0), gr.at[layer, 3])
        to_partner(2, xp)
        run(f"g{layer}b")
        wait(big.at[partner], pr.at[layer, 0])
        arrived(partner)
        for i, d in enumerate((-1, 1)):
            arrived(at_x(d))
            wait(big.at[at_x(d, 1)], pr.at[layer, 1 + i])
            arrived(at_x(d, 1))
        run(f"g{layer}c")
        far = at_x(2)
        wait(half_of(far, 0), gr.at[layer, 4])
        wait(half_of(far, 1), gr.at[layer, 5])
        to_partner(3, far)
        arrived(far)
        wait(big.at[at_x(2, 1)], pr.at[layer, 3])
        arrived(at_x(2, 1))

    for t in range(3, 9):
        run(f"t{t}")
    have(0)

    def project(q, _):
        acc[...] += jnp.dot(xg[q], wrows(0, q), preferred_element_type=F32)
        return 0

    lax.fori_loop(0, n_tp, project, 0)
    hidden = layer_front(0)
    ss[...] = jnp.zeros_like(ss)
    acc[...] = jnp.zeros_like(acc)

    def absorb(q):
        acc[...] += jnp.dot(scaled(1, x1[q], q), wrows(2, q), preferred_element_type=F32)

    def token_chunk():
        return tokens[:, pl.ds(pl.multiple_of(tp * cw, cw), cw)]

    layer_back(0, hidden, token_chunk, x1, absorb)

    hidden = layer_front(1)

    def write_out(q):
        pltpu.make_async_copy(
            outb.at[q], out.at[:, pl.ds(pl.multiple_of(q * cw, cw), cw)], o_sem.at[q]
        ).start()

    layer_back(1, hidden, lambda: x1[tp], outb, write_out)

    for q in range(n_tp):
        pltpu.make_async_copy(outb.at[q], out.at[:, q * cw : (q + 1) * cw], o_sem.at[q]).wait()
    for m in range(4):
        n_hops = n_z - 1
        wait(wbuf.at[m, :, 0 : n_hops * 5 * blk // 2], z_send.at[m])
        wait(wbuf.at[m, :, 0 : (3 + 3 * n_z) * blk // 2], y_send.at[m])
    wait(docs, d_sem.at[0])
    for layer in range(2):
        wait(cbuf.at[layer], c_send.at[layer])
        for j in range(4):
            wait(send_d.at[layer, j], ds.at[layer, j])
            wait(outb.at[j], ps.at[layer, j])
        for j in range(6):
            wait(outb.at[j, 0:hr, :], gs.at[layer, j])
            wait(send_x.at[layer, j], xs.at[layer, j])


def per_device(
    n_sp, tokens, documents, norm_gain, in_weight, conv_taps, conv_bias, recur_gate, input_gate,
    recur_bias, input_bias, decay_param, out_weight,
):
    rows, width = tokens.shape
    layers, blk, chans = in_weight.shape
    n_tp = 2 * NX
    cw = width // n_tp
    hr = rows // 2
    flat = (layers, chans, recur_gate.shape[3])
    vmem = pl.BlockSpec(memory_space=pltpu.VMEM)
    big = pltpu.VMEM((n_tp, rows, cw), BF16)
    square = pltpu.VMEM((rows, chans), F32)
    lanes = pltpu.VMEM((chans // 128, rows, 128), F32)
    strided = pltpu.VMEM((rows // 8, 8, chans), F32)
    dma = pltpu.SemaphoreType.DMA
    scratch = [
        pltpu.VMEM((4, 2, width, chans // 2), BF16),
        pltpu.VMEM((1, rows), jnp.int32),
        pltpu.VMEM((rows + 8, 128), F32),
        pltpu.VMEM((3, rows, 128), F32),
        pltpu.VMEM((layers, chans, 2 * chans), BF16),
        big,
        big,
        big,
        square,
        pltpu.VMEM((rows, 128), F32),
        pltpu.VMEM((rows + 8, chans), F32),
        pltpu.VMEM((layers, 8, chans), F32),
        lanes,
        lanes,
        strided,
        strided,
        lanes,
        pltpu.VMEM((layers, 2, chans), F32),
        pltpu.VMEM((layers, BACK, 2, chans), F32),
        pltpu.VMEM((layers, 4, rows, cw), BF16),
        pltpu.VMEM((layers, 4, rows, cw), BF16),
        pltpu.VMEM((layers, 6, hr, cw), BF16),
        pltpu.VMEM((layers, 6, hr, cw), BF16),
        pltpu.VMEM((rows, cw), F32),
        pltpu.VMEM((rows, cw), F32),
        pltpu.VMEM((4, rows, cw), F32),
        dma((4, 2, n_sp // NY // 2 + 1, 2)),
        dma((4, 2)),
        dma((4,)),
        dma((4,)),
        dma((2,)),
        dma((layers, 2)),
        dma((layers, BACK)),
        dma((layers,)),
        dma((layers, 4)),
        dma((layers, 4)),
        dma((layers, 6)),
        dma((layers, 6)),
        dma((layers, 6)),
        dma((layers, 6)),
        dma((layers, 4)),
        dma((layers, 4)),
        dma((n_tp,)),
    ]
    return pl.pallas_call(
        functools.partial(kernel, n_sp),
        out_shape=jax.ShapeDtypeStruct((rows, width), BF16),
        in_specs=[vmem] * 12,
        out_specs=pl.BlockSpec(memory_space=pl.ANY),
        scratch_shapes=scratch,
        compiler_params=pltpu.CompilerParams(
            collective_id=0, has_side_effects=True, vmem_limit_bytes=56 * 1024 * 1024
        ),
    )(
        documents.reshape(1, rows), tokens, norm_gain, in_weight, conv_taps, conv_bias,
        recur_gate.reshape(flat), input_gate.reshape(flat), recur_bias, input_bias, decay_param, jnp.swapaxes(out_weight, 1, 2),
    )


def solution(mesh):
    return jax.shard_map(
        functools.partial(per_device, mesh.shape["sp"]),
        mesh=mesh,
        in_specs=(
            P("sp", None),
            P("sp"),
            P(),
            P(None, "sp", "tp"),
            P(None, None, "tp"),
            P(None, "tp"),
            P(None, "tp", None, None),
            P(None, "tp", None, None),
            P(None, "tp"),
            P(None, "tp"),
            P(None, "tp"),
            P(None, "tp", "sp"),
        ),
        out_specs=P("sp", None),
        check_vma=False,
    )
```

```python
import functools

import jax
import jax.numpy as jnp
from jax import lax
from jax.experimental import pallas as pl
from jax.experimental.pallas import tpu as pltpu
from jax.sharding import PartitionSpec as P

RG_C = 8.0
EPS = 0.1
MESH = pl.DeviceIdType.MESH
F32 = jnp.float32
BF16 = jnp.bfloat16
NY = 4
NX = 4
BACK = 8
SCHEDULE = {
    "w0": [(0, 0)],
    "w1": [(0, 1), (1, 0)],
    "w2": [(0, 2), (1, 1)],
    "w3": [(0, 3), (1, 2)],
    "w4": [(0, 4), (1, 3)],
    "w5": [(0, 5), (1, 4), (2, 0)],
    "w6": [(0, 6), (1, 5), (2, 1)],
    "w7": [(0, 7), (1, 6), (2, 2), (3, 0)],
    "w8": [(0, 8), (1, 7), (2, 3), (3, 1)],
    "hp": [(1, 8), (2, 4), (3, 2)],
    "f0c": [(2, 5), (3, 3)],
    "f0d": [(2, 6), (3, 4)],
    "b0c": [(2, 7), (3, 5)],
    "b0d": [(2, 8), (3, 6)],
    "g0a": [(3, 7)],
    "g0h": [(3, 8)],
}
TAIL = 16


def nt_dot(a, b):
    return lax.dot_general(a, b, (((1,), (1,)), ((), ())), preferred_element_type=F32)


def kernel(
    n_sp, docs, tokens, gain, w_in, taps, conv_bias, rgate, igate, rbias, ibias, decay, w_out, out,
    wbuf, pdoc, dext, masks, gm, xg, x1, outb, acc, ss, ext, tail, a_s, b_s, h_s, p_s, hid,
    cown, cbuf, send_d, recv_d, send_x, recv_x, keep, own, part,
    z0_recv, z_recv, y_recv, z_send, y_send, d_sem, t_sem, c_recv, c_send, dr, ds, xr, xs, gr, gs, pr, ps, o_sem,
):
    rows, width = tokens.shape
    chans = taps.shape[2]
    blk = w_in.shape[1]
    half_l = chans // 2
    n_tp = 2 * NX
    cw = width // n_tp
    hr = rows // 2
    segs = 8
    steps = rows // segs
    n_z = n_sp // NY
    sp = lax.axis_index("sp")
    tp = lax.axis_index("tp")
    z, y = sp // NY, lax.rem(sp, NY)
    x, core = tp // 2, lax.rem(tp, 2)

    def at_y(d):
        return z * NY + lax.rem(y + d + NY, NY)

    def at_z(d):
        return lax.rem(z + d + n_z, n_z) * NY + y

    def at_sp(d):
        return lax.rem(sp + d + n_sp, n_sp)

    def at_x(d, c=0):
        return lax.rem(x + d + NX, NX) * 2 + (core if c == 0 else 1 - core)

    partner = x * 2 + (1 - core)
    xp, xm = at_x(1), at_x(-1)

    def rcopy(src, dst, ssem, rsem, to_sp, to_tp):
        pltpu.make_async_remote_copy(
            src_ref=src, dst_ref=dst, send_sem=ssem, recv_sem=rsem,
            device_id=(to_sp, to_tp), device_id_type=MESH,
        ).start()

    def wait(ref, sem):
        pltpu.make_async_copy(ref, ref, sem).wait()

    barrier = pltpu.get_barrier_semaphore()
    partners = [(at_y(1), tp), (at_y(-1), tp), (at_y(2), tp), (at_z(1), tp), (at_z(-1), tp)]
    partners += [(sp, xp), (sp, xm), (sp, partner)]
    partners += [(at_sp(d), tp) for k in range(2, BACK + 1) for d in (k, -k)]
    partners += [(at_sp(d), lax.rem(tp + k, n_tp)) for k in range(n_tp) for d in (1, -1)]
    for to_sp, to_tp in partners:
        pl.semaphore_signal(barrier, inc=1, device_id=(to_sp, to_tp), device_id_type=MESH)

    mine = pl.ds(pl.multiple_of(sp * blk, blk), blk)
    for layer in range(2):
        w = w_in[layer]
        wt = w_out[layer]
        for h in range(2):
            lanes = slice(h * half_l, (h + 1) * half_l)
            wbuf[2 * layer, h, mine, :] = w[:, lanes]
            wbuf[2 * layer + 1, h, mine, :] = wt[:, lanes]

    pl.semaphore_wait(barrier, len(partners))

    def block_rows(zz, yy):
        return pl.ds(pl.multiple_of((zz * NY + yy) * blk, blk), blk)

    def z_rows(zz):
        return pl.ds(pl.multiple_of(zz * NY * blk, NY * blk), NY * blk)

    def last_step(m, d):
        full = n_z // 2
        return full if (m + d) % 2 == 0 else full - 1

    def start_y(m):
        for d in (1, -1, 2):
            for h in range(2):
                piece = wbuf.at[m, h, mine, :]
                rcopy(piece, piece, y_send.at[m], y_recv.at[m, h], at_y(d), tp)

    def pieces(m, zz):
        own_col = block_rows(zz, y)
        if m == 0:
            parts = [wbuf.at[m, 1, own_col, :], wbuf.at[m, 0, own_col, :]]
            parts += [wbuf.at[m, 0, block_rows(zz, lax.rem(y + dy + NY, NY)), :] for dy in (1, -1, 2)]
            return parts
        return [wbuf.at[m, 1, own_col, :], wbuf.at[m, 0, z_rows(zz), :]]

    def pass_on(m, d, s, zz, i):
        piece = pieces(m, zz)[i]
        sem = z0_recv.at[d, s, i] if m == 0 else z_recv.at[m - 1, d, s, i]
        rcopy(piece, piece, z_send.at[m], sem, at_z(1 if d == 0 else -1), tp)

    def tick(m, s):
        count = 5 if m == 0 else 2
        if s == 0:
            early = 2 if m == 0 else 1
            for i in range(early):
                for d in range(2):
                    pass_on(m, d, 1, z, i)
            start_y(m)
            wait(wbuf.at[m, 0, 0 : 3 * blk], y_recv.at[m, 0])
            for i in range(early, count):
                for d in range(2):
                    pass_on(m, d, 1, z, i)
            return
        live = [d for d in range(2) if s <= last_step(m, d)]
        zs = {0: lax.rem(z - s + n_z, n_z), 1: lax.rem(z + s, n_z)}
        for i in range(count):
            for d in live:
                sem = z0_recv.at[d, s, i] if m == 0 else z_recv.at[m - 1, d, s, i]
                wait(wbuf.at[m, 0, 0 : (4 * blk if m > 0 and i == 1 else blk)], sem)
                if s < last_step(m, d):
                    pass_on(m, d, s + 1, zs[d], i)
                if i == 0:
                    piece = pieces(m, zs[d])[0]
                    for dy in (1, -1, 2):
                        rcopy(piece, piece, y_send.at[m], y_recv.at[m, 1], at_y(dy), tp)

    def run(point):
        for m, step in SCHEDULE.get(point, ()):
            tick(m, step)

    def have(m):
        wait(wbuf.at[m, 0, 0 : (n_z * 3) * blk], y_recv.at[m, 1])

    def wrows(m, q):
        r = pl.ds(pl.multiple_of(q * cw, cw), cw)
        return jnp.concatenate([wbuf[m, 0, r, :], wbuf[m, 1, r, :]], axis=1)

    rcopy(docs, pdoc, d_sem.at[0], d_sem.at[1], at_sp(1), tp)
    rcopy(tokens.at[rows - TAIL :, :], tail.at[0], t_sem.at[0, 0], t_sem.at[0, 1], at_sp(1), tp)
    run("w0")

    ss[...] = jnp.zeros_like(ss)
    acc[...] = jnp.zeros_like(acc)

    def scaled(layer, values, q):
        columns = pl.ds(pl.multiple_of(q * cw, cw), cw)
        v = jnp.concatenate([tail[layer, :, columns].astype(F32), values.astype(F32)], axis=0)
        sq = v * v
        part = sq[:, 0:128]
        for i in range(1, cw // 128):
            part = part + sq[:, i * 128 : (i + 1) * 128]
        ss[...] += part
        g = gain[layer : layer + 1, columns]
        return (v * g).astype(BF16)

    def prepare(q, _):
        xg[q] = scaled(0, tokens[:, pl.ds(pl.multiple_of(q * cw, cw), cw)], q)
        return 0

    wait(tail.at[0], t_sem.at[0, 1])
    lax.fori_loop(0, n_tp, prepare, 0)
    run("w1")

    bd = rgate.shape[2]
    spread = (
        lax.rem(lax.broadcasted_iota(jnp.int32, (bd, chans), 1), bd)
        == lax.broadcasted_iota(jnp.int32, (bd, chans), 0)
    ).astype(BF16)
    on_block = (
        lax.broadcasted_iota(jnp.int32, (chans, chans), 0) // bd
        == lax.broadcasted_iota(jnp.int32, (chans, chans), 1) // bd
    )
    for layer in range(2):
        for i, g in enumerate((rgate, igate)):
            tiled = jnp.dot(g[layer], spread, preferred_element_type=F32)
            gm[layer, :, i * chans : (i + 1) * chans] = jnp.where(on_block, tiled, 0.0).astype(BF16)
    run("w2")

    wait(pdoc, d_sem.at[1])
    eye_r = (
        lax.broadcasted_iota(jnp.int32, (rows, rows), 0) == lax.broadcasted_iota(jnp.int32, (rows, rows), 1)
    ).astype(BF16)
    own_docs = jnp.broadcast_to(docs[...], (128, rows)).astype(F32).astype(BF16)
    prev_docs = jnp.broadcast_to(pdoc[...], (128, rows)).astype(F32).astype(BF16)
    dext[8:, :] = nt_dot(eye_r, own_docs)
    before = nt_dot(eye_r[rows - 8 :, :], prev_docs)
    first_dev = jnp.broadcast_to((sp == 0).astype(F32), (8, 128))
    dext[0:8, :] = before * (1.0 - first_dev) - first_dev
    for k in range(1, 4):
        masks[k - 1] = (dext[8 - k : 8 - k + rows, :] == dext[8:, :]).astype(F32)

    def put(ref, value):
        for i in range(chans // 128):
            ref[i] = value[:, i * 128 : (i + 1) * 128]

    def across(ref, j):
        return jnp.concatenate(
            [ref[i, pl.ds(j, segs, stride=steps), :] for i in range(chans // 128)], axis=1
        )

    def layer_front(layer):
        r = lax.rsqrt(jnp.sum(ss[...], axis=1, keepdims=True) * (1.0 / width) + EPS)
        ext[...] = (acc[...] * r).astype(BF16).astype(F32)
        run(f"f{layer}a")

        def wide(mask):
            return jnp.concatenate([mask] * (chans // 128), axis=1)

        conv = conv_bias[layer : layer + 1, :] + taps[layer, 0:1, :] * ext[TAIL:, :]
        for k in range(1, 4):
            conv = conv + wide(masks[k - 1]) * (taps[layer, k : k + 1, :] * ext[TAIL - k : TAIL - k + rows, :])
        conv_b = conv.astype(BF16)
        conv_f = conv_b.astype(F32)
        logits = jnp.dot(conv_b, gm[layer], preferred_element_type=F32)
        rr = jax.nn.sigmoid(logits[:, :chans] + rbias[layer : layer + 1, :])
        ir = jax.nn.sigmoid(logits[:, chans:] + ibias[layer : layer + 1, :])
        dp = decay[layer : layer + 1, :]
        soft = jnp.maximum(-dp, 0.0) + jnp.log1p(jnp.exp(-jnp.abs(dp)))
        log_decay = (-RG_C * soft) * rr
        put(a_s, jnp.exp(log_decay) * wide(masks[0]))
        u = -2.0 * log_decay
        series = 1.0 - u * (1.0 / 8.0)
        for n in (7, 6, 5, 4, 3, 2):
            series = 1.0 - (u * (1.0 / n)) * series
        gone = jnp.where(u < 0.35, u * series, 1.0 - jnp.exp(-u))
        put(b_s, jnp.sqrt(jnp.maximum(gone, 0.0)) * (ir * conv_f))
        h = jnp.zeros((segs, chans), F32)
        p = jnp.ones((segs, chans), F32)
        for j in range(steps):
            a_j = across(a_s, j)
            h = a_j * h + across(b_s, j)
            p = p * a_j
            h_s[j] = h
            p_s[j] = p
        al = jnp.ones((1, chans), F32)
        be = jnp.zeros((1, chans), F32)
        als, bes = [al], [be]
        for s in range(segs):
            ps_, hs_ = p[s : s + 1, :], h[s : s + 1, :]
            be = ps_ * be + hs_
            al = ps_ * al
            als.append(al)
            bes.append(be)
        cown[layer, 0:1, :] = al
        cown[layer, 1:2, :] = be
        for k in range(1, BACK + 1):
            rcopy(cown.at[layer], cbuf.at[layer, k - 1], c_send.at[layer], c_recv.at[layer, k - 1], at_sp(k), tp)
        run(f"f{layer}c")
        c_in = jnp.zeros((1, chans), F32)
        for k in range(BACK, 0, -1):
            wait(cbuf.at[layer, k - 1], c_recv.at[layer, k - 1])
            c_in = cbuf[layer, k - 1, 0:1, :] * c_in + cbuf[layer, k - 1, 1:2, :]
        run(f"f{layer}d")
        carry = jnp.concatenate([als[s] * c_in + bes[s] for s in range(segs)], axis=0)
        for j in range(steps):
            value = h_s[j] + p_s[j] * carry
            for i in range(chans // 128):
                hid[i, pl.ds(j, segs, stride=steps), :] = value[:, i * 128 : (i + 1) * 128]
        return jnp.concatenate([hid[i].astype(BF16) for i in range(chans // 128)], axis=1)

    def layer_back(layer, hidden, state_chunk, big, arrived):
        m = 2 * layer + 1
        have(m)
        order = (2, 1, -1, 0)

        def for_partner(j):
            send_d[layer, j] = nt_dot(hidden, wrows(m, at_x(order[j], 1))).astype(BF16)
            rcopy(send_d.at[layer, j], recv_d.at[layer, j], ds.at[layer, j], dr.at[layer, j], sp, partner)

        def for_self(j):
            part[j] = nt_dot(hidden, wrows(m, at_x(order[j])))

        def of_chip(j):
            wait(recv_d.at[layer, j], dr.at[layer, j])
            return part[j] + recv_d[layer, j].astype(F32)

        def send_half(i, value, to):
            send_x[layer, i] = value.astype(BF16)
            rcopy(send_x.at[layer, i], recv_x.at[layer, i], xs.at[layer, i], xr.at[layer, i], sp, to)

        for_partner(0)
        for_self(0)
        for_partner(1)
        both = of_chip(0)
        send_half(0, both[:hr], xp)
        send_half(1, both[hr:], xm)
        for_self(1)
        for_partner(2)
        run(f"b{layer}b")
        both = of_chip(1)
        send_half(2, both[hr:], xp)
        keep[:hr, :] = both[:hr]
        for_self(2)
        for_partner(3)
        both = of_chip(2)
        send_half(3, both[:hr], xm)
        keep[hr:, :] = both[hr:]
        for_self(3)
        own[...] = of_chip(3) + state_chunk().astype(F32)
        run(f"b{layer}c")
        for i, to in ((0, xp), (1, xm)):
            half = slice(0, hr) if i == 0 else slice(hr, rows)
            wait(recv_x.at[layer, i], xr.at[layer, i])
            send_half(4 + i, keep[half, :] + recv_x[layer, i].astype(F32), to)
        run(f"b{layer}d")
        for i in (2, 3):
            wait(recv_x.at[layer, i], xr.at[layer, i])
        top = own[:hr, :] + recv_x[layer, 3].astype(F32)
        bottom = own[hr:, :] + recv_x[layer, 2].astype(F32)

        def half_of(q, h):
            return big.at[q, h * hr : (h + 1) * hr, :]

        def to_x(i, q, h, to):
            rcopy(half_of(q, h), half_of(q, h), gs.at[layer, i], gr.at[layer, i], sp, to)

        def to_partner(i, q):
            rcopy(big.at[q], big.at[q], ps.at[layer, i], pr.at[layer, i], sp, partner)

        wait(recv_x.at[layer, 4], xr.at[layer, 4])
        big[tp, 0:hr, :] = (top + recv_x[layer, 4].astype(F32)).astype(BF16)
        to_x(0, tp, 0, xp)
        wait(recv_x.at[layer, 5], xr.at[layer, 5])
        big[tp, hr:rows, :] = (bottom + recv_x[layer, 5].astype(F32)).astype(BF16)
        to_x(1, tp, 1, xm)
        to_x(2, tp, 1, xp)
        to_x(3, tp, 0, xm)
        to_partner(0, tp)
        if layer == 0:
            for k in range(n_tp):
                rcopy(
                    big.at[tp, rows - TAIL : rows, :],
                    tail.at[1, :, pl.ds(pl.multiple_of(tp * cw, cw), cw)],
                    t_sem.at[1, 0], t_sem.at[1, 1], at_sp(1), lax.rem(tp + k, n_tp),
                )
        held = [tp]
        run(f"g{layer}a")
        wait(half_of(xm, 0), gr.at[layer, 0])
        to_x(4, xm, 0, xp)
        wait(half_of(xp, 1), gr.at[layer, 1])
        to_x(5, xp, 1, xm)
        run(f"g{layer}h")
        wait(half_of(xm, 1), gr.at[layer, 2])
        to_partner(1, xm)
        wait(half_of(xp, 0), gr.at[layer, 3])
        to_partner(2, xp)
        run(f"g{layer}b")
        wait(big.at[partner], pr.at[layer, 0])
        held += [partner, xm, xp]
        for i, d in enumerate((-1, 1)):
            wait(big.at[at_x(d, 1)], pr.at[layer, 1 + i])
            held.append(at_x(d, 1))
        run(f"g{layer}c")
        if layer == 0:
            have(2)
            wait(tail.at[1], t_sem.at[1, 1])
        for q in held:
            arrived(q)
        far = at_x(2)
        wait(half_of(far, 0), gr.at[layer, 4])
        wait(half_of(far, 1), gr.at[layer, 5])
        to_partner(3, far)
        arrived(far)
        wait(big.at[at_x(2, 1)], pr.at[layer, 3])
        arrived(at_x(2, 1))

    for t in range(3, 9):
        run(f"w{t}")
    have(0)
    run("hp")

    def project(q, _):
        acc[...] += jnp.dot(xg[q], wrows(0, q), preferred_element_type=F32)
        return 0

    lax.fori_loop(0, n_tp, project, 0)
    hidden = layer_front(0)
    ss[...] = jnp.zeros_like(ss)
    acc[...] = jnp.zeros_like(acc)

    def absorb(q):
        acc[...] += jnp.dot(scaled(1, x1[q], q), wrows(2, q), preferred_element_type=F32)

    def token_chunk():
        return tokens[:, pl.ds(pl.multiple_of(tp * cw, cw), cw)]

    layer_back(0, hidden, token_chunk, x1, absorb)

    hidden = layer_front(1)

    def write_out(q):
        pltpu.make_async_copy(
            outb.at[q], out.at[:, pl.ds(pl.multiple_of(q * cw, cw), cw)], o_sem.at[q]
        ).start()

    layer_back(1, hidden, lambda: x1[tp], outb, write_out)

    for q in range(n_tp):
        pltpu.make_async_copy(outb.at[q], out.at[:, q * cw : (q + 1) * cw], o_sem.at[q]).wait()
    for m in range(4):
        n_hops = n_z - 1
        wait(wbuf.at[m, :, 0 : n_hops * 5 * blk // 2], z_send.at[m])
        wait(wbuf.at[m, :, 0 : (3 + 3 * n_z) * blk // 2], y_send.at[m])
    wait(docs, d_sem.at[0])
    for layer in range(2):
        wait(tail.at[layer], t_sem.at[layer, 0])
        wait(cbuf.at[layer], c_send.at[layer])
        for j in range(4):
            wait(send_d.at[layer, j], ds.at[layer, j])
            wait(outb.at[j], ps.at[layer, j])
        for j in range(6):
            wait(outb.at[j, 0:hr, :], gs.at[layer, j])
            wait(send_x.at[layer, j], xs.at[layer, j])


def per_device(
    n_sp, tokens, documents, norm_gain, in_weight, conv_taps, conv_bias, recur_gate, input_gate,
    recur_bias, input_bias, decay_param, out_weight,
):
    rows, width = tokens.shape
    layers, blk, chans = in_weight.shape
    n_tp = 2 * NX
    cw = width // n_tp
    hr = rows // 2
    flat = (layers, chans, recur_gate.shape[3])
    vmem = pl.BlockSpec(memory_space=pltpu.VMEM)
    big = pltpu.VMEM((n_tp, rows, cw), BF16)
    lanes = pltpu.VMEM((chans // 128, rows, 128), F32)
    strided = pltpu.VMEM((rows // 8, 8, chans), F32)
    dma = pltpu.SemaphoreType.DMA
    scratch = [
        pltpu.VMEM((4, 2, width, chans // 2), BF16),
        pltpu.VMEM((1, rows), jnp.int32),
        pltpu.VMEM((rows + 8, 128), F32),
        pltpu.VMEM((3, rows, 128), F32),
        pltpu.VMEM((layers, chans, 2 * chans), BF16),
        pltpu.VMEM((n_tp, rows + TAIL, cw), BF16),
        big,
        big,
        pltpu.VMEM((rows + TAIL, chans), F32),
        pltpu.VMEM((rows + TAIL, 128), F32),
        pltpu.VMEM((rows + TAIL, chans), F32),
        pltpu.VMEM((layers, TAIL, width), BF16),
        lanes,
        lanes,
        strided,
        strided,
        lanes,
        pltpu.VMEM((layers, 2, chans), F32),
        pltpu.VMEM((layers, BACK, 2, chans), F32),
        pltpu.VMEM((layers, 4, rows, cw), BF16),
        pltpu.VMEM((layers, 4, rows, cw), BF16),
        pltpu.VMEM((layers, 6, hr, cw), BF16),
        pltpu.VMEM((layers, 6, hr, cw), BF16),
        pltpu.VMEM((rows, cw), F32),
        pltpu.VMEM((rows, cw), F32),
        pltpu.VMEM((4, rows, cw), F32),
        dma((2, n_sp // NY // 2 + 1, 5)),
        dma((3, 2, n_sp // NY // 2 + 1, 2)),
        dma((4, 2)),
        dma((4,)),
        dma((4,)),
        dma((2,)),
        dma((layers, 2)),
        dma((layers, BACK)),
        dma((layers,)),
        dma((layers, 4)),
        dma((layers, 4)),
        dma((layers, 6)),
        dma((layers, 6)),
        dma((layers, 6)),
        dma((layers, 6)),
        dma((layers, 4)),
        dma((layers, 4)),
        dma((n_tp,)),
    ]
    return pl.pallas_call(
        functools.partial(kernel, n_sp),
        out_shape=jax.ShapeDtypeStruct((rows, width), BF16),
        in_specs=[vmem] * 12,
        out_specs=pl.BlockSpec(memory_space=pl.ANY),
        scratch_shapes=scratch,
        compiler_params=pltpu.CompilerParams(
            collective_id=0, has_side_effects=True, vmem_limit_bytes=56 * 1024 * 1024
        ),
    )(
        documents.reshape(1, rows), tokens, norm_gain, in_weight, conv_taps, conv_bias,
        recur_gate.reshape(flat), input_gate.reshape(flat), recur_bias, input_bias, decay_param, jnp.swapaxes(out_weight, 1, 2),
    )


def solution(mesh):
    return jax.shard_map(
        functools.partial(per_device, mesh.shape["sp"]),
        mesh=mesh,
        in_specs=(
            P("sp", None),
            P("sp"),
            P(),
            P(None, "sp", "tp"),
            P(None, None, "tp"),
            P(None, "tp"),
            P(None, "tp", None, None),
            P(None, "tp", None, None),
            P(None, "tp"),
            P(None, "tp"),
            P(None, "tp"),
            P(None, "tp", "sp"),
        ),
        out_specs=P("sp", None),
        check_vma=False,
    )
```

```python
import functools

import jax
import jax.numpy as jnp
from jax import lax
from jax.experimental import pallas as pl
from jax.experimental.pallas import tpu as pltpu
from jax.sharding import PartitionSpec as P

RG_C = 8.0
EPS = 0.1
MESH = pl.DeviceIdType.MESH
F32 = jnp.float32
BF16 = jnp.bfloat16
NY = 4
NX = 4
BACK = 8
SCHEDULE = {
    "w0": [(0, 0)],
    "w1": [(0, 1), (1, 0)],
    "w2": [(0, 2), (1, 1)],
    "w3": [(0, 3), (1, 2)],
    "w4": [(0, 4), (1, 3)],
    "w5": [(0, 5), (1, 4), (2, 0)],
    "w6": [(0, 6), (1, 5), (2, 1)],
    "w7": [(0, 7), (1, 6), (2, 2), (3, 0)],
    "w8": [(0, 8), (1, 7), (2, 3), (3, 1)],
    "hp": [(1, 8), (2, 4), (3, 2)],
    "f0c": [(2, 5), (3, 3)],
    "f0d": [(2, 6), (3, 4)],
    "b0c": [(2, 7), (3, 5)],
    "b0d": [(2, 8), (3, 6)],
    "g0a": [(3, 7)],
    "g0h": [(3, 8)],
}
TAIL = 16


def nt_dot(a, b):
    return lax.dot_general(a, b, (((1,), (1,)), ((), ())), preferred_element_type=F32)


def kernel(
    n_sp, docs, tokens, gain, w_in, taps, conv_bias, rgate, igate, rbias, ibias, decay, w_out, out,
    wbuf, pdoc, dext, masks, gm, xg, x1, outb, acc, ss, ext, tail, a_s, b_s, h_s, p_s, hid,
    cown, cbuf, send_d, recv_d, send_x, recv_x, keep, own, part,
    z0_recv, z_recv, y_recv, z_send, y_send, d_sem, t_sem, c_recv, c_send, dr, ds, xr, xs, gr, gs, pr, ps, o_sem,
):
    rows, width = tokens.shape
    chans = taps.shape[2]
    blk = w_in.shape[1]
    half_l = chans // 2
    n_tp = 2 * NX
    cw = width // n_tp
    hr = rows // 2
    segs = 8
    steps = rows // segs
    n_z = n_sp // NY
    sp = lax.axis_index("sp")
    tp = lax.axis_index("tp")
    z, y = sp // NY, lax.rem(sp, NY)
    x, core = tp // 2, lax.rem(tp, 2)

    def at_y(d):
        return z * NY + lax.rem(y + d + NY, NY)

    def at_z(d):
        return lax.rem(z + d + n_z, n_z) * NY + y

    def at_sp(d):
        return lax.rem(sp + d + n_sp, n_sp)

    def at_x(d, c=0):
        return lax.rem(x + d + NX, NX) * 2 + (core if c == 0 else 1 - core)

    partner = x * 2 + (1 - core)
    xp, xm = at_x(1), at_x(-1)

    def rcopy(src, dst, ssem, rsem, to_sp, to_tp):
        pltpu.make_async_remote_copy(
            src_ref=src, dst_ref=dst, send_sem=ssem, recv_sem=rsem,
            device_id=(to_sp, to_tp), device_id_type=MESH,
        ).start()

    def wait(ref, sem):
        pltpu.make_async_copy(ref, ref, sem).wait()

    barrier = pltpu.get_barrier_semaphore()
    partners = [(at_y(1), tp), (at_y(-1), tp), (at_y(2), tp), (at_z(1), tp), (at_z(-1), tp)]
    partners += [(sp, xp), (sp, xm), (sp, partner)]
    partners += [(at_sp(d), tp) for k in range(2, BACK + 1) for d in (k, -k)]
    partners += [(at_sp(d), lax.rem(tp + k, n_tp)) for k in range(n_tp) for d in (1, -1)]
    for to_sp, to_tp in partners:
        pl.semaphore_signal(barrier, inc=1, device_id=(to_sp, to_tp), device_id_type=MESH)

    mine = pl.ds(pl.multiple_of(sp * blk, blk), blk)
    for layer in range(2):
        w = w_in[layer]
        wt = w_out[layer]
        for h in range(2):
            lanes = slice(h * half_l, (h + 1) * half_l)
            wbuf[2 * layer, h, mine, :] = w[:, lanes]
            wbuf[2 * layer + 1, h, mine, :] = wt[:, lanes]

    pl.semaphore_wait(barrier, len(partners))

    def block_rows(zz, yy):
        return pl.ds(pl.multiple_of((zz * NY + yy) * blk, blk), blk)

    def z_rows(zz):
        return pl.ds(pl.multiple_of(zz * NY * blk, NY * blk), NY * blk)

    def last_step(m, d):
        full = n_z // 2
        return full if (m + d) % 2 == 0 else full - 1

    def start_y(m):
        for d in (1, -1, 2):
            for h in range(2):
                piece = wbuf.at[m, h, mine, :]
                rcopy(piece, piece, y_send.at[m], y_recv.at[m, h], at_y(d), tp)

    def pieces(m, zz):
        own_col = block_rows(zz, y)
        if m == 0:
            parts = [wbuf.at[m, 1, own_col, :], wbuf.at[m, 0, own_col, :]]
            parts += [wbuf.at[m, 0, block_rows(zz, lax.rem(y + dy + NY, NY)), :] for dy in (1, -1, 2)]
            return parts
        return [wbuf.at[m, 1, own_col, :], wbuf.at[m, 0, z_rows(zz), :]]

    def pass_on(m, d, s, zz, i):
        piece = pieces(m, zz)[i]
        sem = z0_recv.at[d, s, i] if m == 0 else z_recv.at[m - 1, d, s, i]
        rcopy(piece, piece, z_send.at[m], sem, at_z(1 if d == 0 else -1), tp)

    def tick(m, s):
        count = 5 if m == 0 else 2
        if s == 0:
            early = 2 if m == 0 else 1
            for i in range(early):
                for d in range(2):
                    pass_on(m, d, 1, z, i)
            start_y(m)
            wait(wbuf.at[m, 0, 0 : 3 * blk], y_recv.at[m, 0])
            for i in range(early, count):
                for d in range(2):
                    pass_on(m, d, 1, z, i)
            return
        live = [d for d in range(2) if s <= last_step(m, d)]
        zs = {0: lax.rem(z - s + n_z, n_z), 1: lax.rem(z + s, n_z)}
        for i in range(count):
            for d in live:
                sem = z0_recv.at[d, s, i] if m == 0 else z_recv.at[m - 1, d, s, i]
                wait(wbuf.at[m, 0, 0 : (4 * blk if m > 0 and i == 1 else blk)], sem)
                if s < last_step(m, d):
                    pass_on(m, d, s + 1, zs[d], i)
                if i == 0:
                    piece = pieces(m, zs[d])[0]
                    for dy in (1, -1, 2):
                        rcopy(piece, piece, y_send.at[m], y_recv.at[m, 1], at_y(dy), tp)

    def run(point):
        for m, step in SCHEDULE.get(point, ()):
            tick(m, step)

    def have(m):
        wait(wbuf.at[m, 0, 0 : (n_z * 3) * blk], y_recv.at[m, 1])

    def wrows(m, q):
        r = pl.ds(pl.multiple_of(q * cw, cw), cw)
        return jnp.concatenate([wbuf[m, 0, r, :], wbuf[m, 1, r, :]], axis=1)

    rcopy(docs, pdoc, d_sem.at[0], d_sem.at[1], at_sp(1), tp)
    rcopy(tokens.at[rows - TAIL :, :], tail.at[0], t_sem.at[0, 0], t_sem.at[0, 1], at_sp(1), tp)
    run("w0")

    ss[...] = jnp.zeros_like(ss)
    acc[...] = jnp.zeros_like(acc)

    def scaled(layer, values, q):
        columns = pl.ds(pl.multiple_of(q * cw, cw), cw)
        v = jnp.concatenate([tail[layer, :, columns].astype(F32), values.astype(F32)], axis=0)
        sq = v * v
        part = sq[:, 0:128]
        for i in range(1, cw // 128):
            part = part + sq[:, i * 128 : (i + 1) * 128]
        ss[...] += part
        g = gain[layer : layer + 1, columns]
        return (v * g).astype(BF16)

    def prepare(q, _):
        xg[q] = scaled(0, tokens[:, pl.ds(pl.multiple_of(q * cw, cw), cw)], q)
        return 0

    wait(tail.at[0], t_sem.at[0, 1])
    lax.fori_loop(0, n_tp, prepare, 0)
    run("w1")

    bd = rgate.shape[2]
    spread = (
        lax.rem(lax.broadcasted_iota(jnp.int32, (bd, chans), 1), bd)
        == lax.broadcasted_iota(jnp.int32, (bd, chans), 0)
    ).astype(BF16)
    on_block = (
        lax.broadcasted_iota(jnp.int32, (chans, chans), 0) // bd
        == lax.broadcasted_iota(jnp.int32, (chans, chans), 1) // bd
    )
    for layer in range(2):
        for i, g in enumerate((rgate, igate)):
            tiled = jnp.dot(g[layer], spread, preferred_element_type=F32)
            gm[layer, :, i * chans : (i + 1) * chans] = jnp.where(on_block, tiled, 0.0).astype(BF16)
    run("w2")

    wait(pdoc, d_sem.at[1])
    eye_r = (
        lax.broadcasted_iota(jnp.int32, (rows, rows), 0) == lax.broadcasted_iota(jnp.int32, (rows, rows), 1)
    ).astype(BF16)
    own_docs = jnp.broadcast_to(docs[...], (128, rows)).astype(F32).astype(BF16)
    prev_docs = jnp.broadcast_to(pdoc[...], (128, rows)).astype(F32).astype(BF16)
    dext[8:, :] = nt_dot(eye_r, own_docs)
    before = nt_dot(eye_r[rows - 8 :, :], prev_docs)
    first_dev = jnp.broadcast_to((sp == 0).astype(F32), (8, 128))
    dext[0:8, :] = before * (1.0 - first_dev) - first_dev
    for k in range(1, 4):
        masks[k - 1] = (dext[8 - k : 8 - k + rows, :] == dext[8:, :]).astype(F32)

    def put(ref, value):
        for i in range(chans // 128):
            ref[i] = value[:, i * 128 : (i + 1) * 128]

    def across(ref, j):
        return jnp.concatenate(
            [ref[i, pl.ds(j, segs, stride=steps), :] for i in range(chans // 128)], axis=1
        )

    def layer_front(layer):
        r = lax.rsqrt(jnp.sum(ss[...], axis=1, keepdims=True) * (1.0 / width) + EPS)
        ext[...] = (acc[...] * r).astype(BF16).astype(F32)
        run(f"f{layer}a")

        def wide(mask):
            return jnp.concatenate([mask] * (chans // 128), axis=1)

        conv = conv_bias[layer : layer + 1, :] + taps[layer, 0:1, :] * ext[TAIL:, :]
        for k in range(1, 4):
            conv = conv + wide(masks[k - 1]) * (taps[layer, k : k + 1, :] * ext[TAIL - k : TAIL - k + rows, :])
        conv_b = conv.astype(BF16)
        conv_f = conv_b.astype(F32)
        logits = jnp.dot(conv_b, gm[layer], preferred_element_type=F32)
        rr = jax.nn.sigmoid(logits[:, :chans] + rbias[layer : layer + 1, :])
        ir = jax.nn.sigmoid(logits[:, chans:] + ibias[layer : layer + 1, :])
        dp = decay[layer : layer + 1, :]
        soft = jnp.maximum(-dp, 0.0) + jnp.log1p(jnp.exp(-jnp.abs(dp)))
        log_decay = (-RG_C * soft) * rr
        put(a_s, jnp.exp(log_decay) * wide(masks[0]))
        u = -2.0 * log_decay
        series = 1.0 - u * (1.0 / 8.0)
        for n in (7, 6, 5, 4, 3, 2):
            series = 1.0 - (u * (1.0 / n)) * series
        gone = jnp.where(u < 0.35, u * series, 1.0 - jnp.exp(-u))
        put(b_s, jnp.sqrt(jnp.maximum(gone, 0.0)) * (ir * conv_f))
        h = jnp.zeros((segs, chans), F32)
        p = jnp.ones((segs, chans), F32)
        for j in range(steps):
            a_j = across(a_s, j)
            h = a_j * h + across(b_s, j)
            p = p * a_j
            h_s[j] = h
            p_s[j] = p
        al = jnp.ones((1, chans), F32)
        be = jnp.zeros((1, chans), F32)
        als, bes = [al], [be]
        for s in range(segs):
            ps_, hs_ = p[s : s + 1, :], h[s : s + 1, :]
            be = ps_ * be + hs_
            al = ps_ * al
            als.append(al)
            bes.append(be)
        cown[layer, 0:1, :] = al
        cown[layer, 1:2, :] = be
        for k in range(1, BACK + 1):
            rcopy(cown.at[layer], cbuf.at[layer, k - 1], c_send.at[layer], c_recv.at[layer, k - 1], at_sp(k), tp)
        run(f"f{layer}c")
        c_in = jnp.zeros((1, chans), F32)
        for k in range(BACK, 0, -1):
            wait(cbuf.at[layer, k - 1], c_recv.at[layer, k - 1])
            c_in = cbuf[layer, k - 1, 0:1, :] * c_in + cbuf[layer, k - 1, 1:2, :]
        run(f"f{layer}d")
        carry = jnp.concatenate([als[s] * c_in + bes[s] for s in range(segs)], axis=0)
        for j in range(steps):
            value = h_s[j] + p_s[j] * carry
            for i in range(chans // 128):
                hid[i, pl.ds(j, segs, stride=steps), :] = value[:, i * 128 : (i + 1) * 128]
        return jnp.concatenate([hid[i].astype(BF16) for i in range(chans // 128)], axis=1)

    def layer_back(layer, hidden, state_chunk, big, arrived):
        m = 2 * layer + 1
        have(m)
        order = (2, 1, -1, 0)

        def for_partner(j):
            send_d[layer, j] = nt_dot(hidden, wrows(m, at_x(order[j], 1))).astype(BF16)
            rcopy(send_d.at[layer, j], recv_d.at[layer, j], ds.at[layer, j], dr.at[layer, j], sp, partner)

        def for_self(j):
            part[j] = nt_dot(hidden, wrows(m, at_x(order[j])))

        def of_chip(j):
            wait(recv_d.at[layer, j], dr.at[layer, j])
            return part[j] + recv_d[layer, j].astype(F32)

        def send_half(i, value, to):
            send_x[layer, i] = value.astype(BF16)
            rcopy(send_x.at[layer, i], recv_x.at[layer, i], xs.at[layer, i], xr.at[layer, i], sp, to)

        for_partner(0)
        for_self(0)
        for_partner(1)
        both = of_chip(0)
        send_half(0, both[:hr], xp)
        send_half(1, both[hr:], xm)
        for_self(1)
        for_partner(2)
        run(f"b{layer}b")
        both = of_chip(1)
        send_half(2, both[hr:], xp)
        keep[:hr, :] = both[:hr]
        for_self(2)
        for_partner(3)
        both = of_chip(2)
        send_half(3, both[:hr], xm)
        keep[hr:, :] = both[hr:]
        for_self(3)
        own[...] = of_chip(3) + state_chunk().astype(F32)
        run(f"b{layer}c")
        for i, to in ((0, xp), (1, xm)):
            half = slice(0, hr) if i == 0 else slice(hr, rows)
            wait(recv_x.at[layer, i], xr.at[layer, i])
            send_half(4 + i, keep[half, :] + recv_x[layer, i].astype(F32), to)
        run(f"b{layer}d")
        for i in (2, 3):
            wait(recv_x.at[layer, i], xr.at[layer, i])
        top = own[:hr, :] + recv_x[layer, 3].astype(F32)
        bottom = own[hr:, :] + recv_x[layer, 2].astype(F32)

        def half_of(q, h):
            return big.at[q, h * hr : (h + 1) * hr, :]

        def to_x(i, q, h, to):
            rcopy(half_of(q, h), half_of(q, h), gs.at[layer, i], gr.at[layer, i], sp, to)

        def to_partner(i, q):
            rcopy(big.at[q], big.at[q], ps.at[layer, i], pr.at[layer, i], sp, partner)

        wait(recv_x.at[layer, 4], xr.at[layer, 4])
        big[tp, 0:hr, :] = (top + recv_x[layer, 4].astype(F32)).astype(BF16)
        to_x(0, tp, 0, xp)
        wait(recv_x.at[layer, 5], xr.at[layer, 5])
        big[tp, hr:rows, :] = (bottom + recv_x[layer, 5].astype(F32)).astype(BF16)
        to_x(1, tp, 1, xm)
        to_x(2, tp, 1, xp)
        to_x(3, tp, 0, xm)
        to_partner(0, tp)
        if layer == 0:
            for k in range(n_tp):
                rcopy(
                    big.at[tp, rows - TAIL : rows, :],
                    tail.at[1, :, pl.ds(pl.multiple_of(tp * cw, cw), cw)],
                    t_sem.at[1, 0], t_sem.at[1, 1], at_sp(1), lax.rem(tp + k, n_tp),
                )
        held = [tp]
        run(f"g{layer}a")
        wait(half_of(xm, 0), gr.at[layer, 0])
        to_x(4, xm, 0, xp)
        wait(half_of(xp, 1), gr.at[layer, 1])
        to_x(5, xp, 1, xm)
        run(f"g{layer}h")
        wait(half_of(xm, 1), gr.at[layer, 2])
        to_partner(1, xm)
        wait(half_of(xp, 0), gr.at[layer, 3])
        to_partner(2, xp)
        run(f"g{layer}b")
        wait(big.at[partner], pr.at[layer, 0])
        held += [partner, xm, xp]
        for i, d in enumerate((-1, 1)):
            wait(big.at[at_x(d, 1)], pr.at[layer, 1 + i])
            held.append(at_x(d, 1))
        run(f"g{layer}c")
        if layer == 0:
            have(2)
            wait(tail.at[1], t_sem.at[1, 1])
        for q in held:
            arrived(q)
        far = at_x(2)
        wait(half_of(far, 0), gr.at[layer, 4])
        wait(half_of(far, 1), gr.at[layer, 5])
        to_partner(3, far)
        arrived(far)
        wait(big.at[at_x(2, 1)], pr.at[layer, 3])
        arrived(at_x(2, 1))

    for t in range(3, 9):
        run(f"w{t}")
    have(0)
    run("hp")

    def project(q, _):
        acc[...] += jnp.dot(xg[q], wrows(0, q), preferred_element_type=F32)
        return 0

    lax.fori_loop(0, n_tp, project, 0)
    hidden = layer_front(0)
    ss[...] = jnp.zeros_like(ss)
    acc[...] = jnp.zeros_like(acc)

    def absorb(q):
        acc[...] += jnp.dot(scaled(1, x1[q], q), wrows(2, q), preferred_element_type=F32)

    def token_chunk():
        return tokens[:, pl.ds(pl.multiple_of(tp * cw, cw), cw)]

    layer_back(0, hidden, token_chunk, x1, absorb)

    hidden = layer_front(1)

    def write_out(q):
        pltpu.make_async_copy(
            outb.at[q], out.at[q], o_sem.at[q]
        ).start()

    layer_back(1, hidden, lambda: x1[tp], outb, write_out)

    for q in range(n_tp):
        pltpu.make_async_copy(outb.at[q], out.at[q], o_sem.at[q]).wait()
    for m in range(4):
        n_hops = n_z - 1
        wait(wbuf.at[m, :, 0 : n_hops * 5 * blk // 2], z_send.at[m])
        wait(wbuf.at[m, :, 0 : (3 + 3 * n_z) * blk // 2], y_send.at[m])
    wait(docs, d_sem.at[0])
    for layer in range(2):
        wait(tail.at[layer], t_sem.at[layer, 0])
        wait(cbuf.at[layer], c_send.at[layer])
        for j in range(4):
            wait(send_d.at[layer, j], ds.at[layer, j])
            wait(outb.at[j], ps.at[layer, j])
        for j in range(6):
            wait(outb.at[j, 0:hr, :], gs.at[layer, j])
            wait(send_x.at[layer, j], xs.at[layer, j])


def per_device(
    n_sp, tokens, documents, norm_gain, in_weight, conv_taps, conv_bias, recur_gate, input_gate,
    recur_bias, input_bias, decay_param, out_weight,
):
    rows, width = tokens.shape
    layers, blk, chans = in_weight.shape
    n_tp = 2 * NX
    cw = width // n_tp
    hr = rows // 2
    flat = (layers, chans, recur_gate.shape[3])
    vmem = pl.BlockSpec(memory_space=pltpu.VMEM)
    big = pltpu.VMEM((n_tp, rows, cw), BF16)
    lanes = pltpu.VMEM((chans // 128, rows, 128), F32)
    strided = pltpu.VMEM((rows // 8, 8, chans), F32)
    dma = pltpu.SemaphoreType.DMA
    scratch = [
        pltpu.VMEM((4, 2, width, chans // 2), BF16),
        pltpu.VMEM((1, rows), jnp.int32),
        pltpu.VMEM((rows + 8, 128), F32),
        pltpu.VMEM((3, rows, 128), F32),
        pltpu.VMEM((layers, chans, 2 * chans), BF16),
        pltpu.VMEM((n_tp, rows + TAIL, cw), BF16),
        big,
        big,
        pltpu.VMEM((rows + TAIL, chans), F32),
        pltpu.VMEM((rows + TAIL, 128), F32),
        pltpu.VMEM((rows + TAIL, chans), F32),
        pltpu.VMEM((layers, TAIL, width), BF16),
        lanes,
        lanes,
        strided,
        strided,
        lanes,
        pltpu.VMEM((layers, 2, chans), F32),
        pltpu.VMEM((layers, BACK, 2, chans), F32),
        pltpu.VMEM((layers, 4, rows, cw), BF16),
        pltpu.VMEM((layers, 4, rows, cw), BF16),
        pltpu.VMEM((layers, 6, hr, cw), BF16),
        pltpu.VMEM((layers, 6, hr, cw), BF16),
        pltpu.VMEM((rows, cw), F32),
        pltpu.VMEM((rows, cw), F32),
        pltpu.VMEM((4, rows, cw), F32),
        dma((2, n_sp // NY // 2 + 1, 5)),
        dma((3, 2, n_sp // NY // 2 + 1, 2)),
        dma((4, 2)),
        dma((4,)),
        dma((4,)),
        dma((2,)),
        dma((layers, 2)),
        dma((layers, BACK)),
        dma((layers,)),
        dma((layers, 4)),
        dma((layers, 4)),
        dma((layers, 6)),
        dma((layers, 6)),
        dma((layers, 6)),
        dma((layers, 6)),
        dma((layers, 4)),
        dma((layers, 4)),
        dma((n_tp,)),
    ]
    chunks = pl.pallas_call(
        functools.partial(kernel, n_sp),
        out_shape=jax.ShapeDtypeStruct((n_tp, rows, cw), BF16),
        in_specs=[vmem] * 12,
        out_specs=pl.BlockSpec(memory_space=pl.ANY),
        scratch_shapes=scratch,
        compiler_params=pltpu.CompilerParams(
            collective_id=0, has_side_effects=True, vmem_limit_bytes=56 * 1024 * 1024
        ),
    )(
        documents.reshape(1, rows), tokens, norm_gain, in_weight, conv_taps, conv_bias,
        recur_gate.reshape(flat), input_gate.reshape(flat), recur_bias, input_bias, decay_param, jnp.swapaxes(out_weight, 1, 2),
    )
    return laid_out(chunks)


def copy_kernel(src, dst, buf, i_sem, o_sem):
    n, rows, cw = buf.shape
    for q in range(n):
        pltpu.make_async_copy(src.at[q], buf.at[q], i_sem.at[q]).start()
    for q in range(n):
        pltpu.make_async_copy(src.at[q], buf.at[q], i_sem.at[q]).wait()
        pltpu.make_async_copy(buf.at[q], dst.at[:, q * cw : (q + 1) * cw], o_sem.at[q]).start()
    for q in range(n):
        pltpu.make_async_copy(buf.at[q], dst.at[:, q * cw : (q + 1) * cw], o_sem.at[q]).wait()


def laid_out(chunks):
    n, rows, cw = chunks.shape
    anywhere = pl.BlockSpec(memory_space=pl.ANY)
    return pl.pallas_call(
        copy_kernel,
        out_shape=jax.ShapeDtypeStruct((rows, n * cw), BF16),
        in_specs=[anywhere],
        out_specs=anywhere,
        scratch_shapes=[
            pltpu.VMEM((n, rows, cw), BF16),
            pltpu.SemaphoreType.DMA((n,)),
            pltpu.SemaphoreType.DMA((n,)),
        ],
    )(chunks)


def solution(mesh):
    return jax.shard_map(
        functools.partial(per_device, mesh.shape["sp"]),
        mesh=mesh,
        in_specs=(
            P("sp", None),
            P("sp"),
            P(),
            P(None, "sp", "tp"),
            P(None, None, "tp"),
            P(None, "tp"),
            P(None, "tp", None, None),
            P(None, "tp", None, None),
            P(None, "tp"),
            P(None, "tp"),
            P(None, "tp"),
            P(None, "tp", "sp"),
        ),
        out_specs=P("sp", None),
        check_vma=False,
    )
```
